512 devices in a mesh: sp: 64 (over z, y), tp: 8 (over x, core).
Axes of the slice: x: 4, y: 4, z: 16, core: 2. Of those that a mesh axis runs over, the one named last changes fastest.
Arguments:
- mixer_in: bfloat16 [32768, 1024], P('sp', 'tp'), may hold values from -6 to 6
- residual: bfloat16 [32768, 2048], P(('sp', 'tp')), may hold values from -6 to 6
- decay_real: float32 [64, 64], P('tp'), may hold values from -2 to 0, as said below
- decay_imag: float32 [64, 64], P('tp'), may hold values from 1 to 200
- log_step: float32 [64], P('tp'), may hold values from -3.9 to -2.5
- in_real: float32 [64, 64, 16], P('tp'), may hold values from -1 to 1
- in_imag: float32 [64, 64, 16], P('tp'), may hold values from -1 to 1
- output_real: float32 [64, 16, 64], P('tp'), may hold values from -0.5 to 0.5
- output_imaginary: float32 [64, 16, 64], P('tp'), may hold values from -0.5 to 0.5
- skip: float32 [1024], P('tp'), may hold values from -4 to 4
- out_proj: bfloat16 [1024, 2048], P('tp'), may hold values from -0.1875 to 0.1875
- norm_gain: float32 [2048], replicated, may hold values from 0.1 to 1.9
- w_gate: bfloat16 [2048, 5632], P('sp', 'tp'), may hold values from -0.125 to 0.125
- w_up: bfloat16 [2048, 5632], P('sp', 'tp'), may hold values from -0.125 to 0.125
- w_down: bfloat16 [5632, 2048], P('tp', 'sp'), may hold values from -0.078125 to 0.078125
Outputs:
- output: bfloat16 [32768, 2048], P(('sp', 'tp'))
The draws below stay inside these ranges and needn't reach their ends.
Inputs may be any that keep to these rules, and one draw needn't show every extreme that they name: `decay_real`: every entry is negative.
All inputs are finite; a program needn't handle non-finite values.
Results may differ from the reference program's by a relative error of at most 0.02.
Values may be sent and summed in bfloat16 or wider, within the bound.
A program may use at most 64 MiB of HBM per device.

```python
import jax
import jax.numpy as jnp
from jax import lax

D = 2048
CH = 1024
GROUP = 16
STATE = 64
FF = 5632
TOK_DEV = 512
GROUPS = 64
TOKENS = 32768
CH_DEV = 128
FF_DEV = 704
N_SP = 64


def draw_decay_real(key, part):
    slow_key, rate_key = jax.random.split(jax.random.fold_in(key, 11))
    slow = jax.random.bernoulli(slow_key, 0.5, (GROUPS, 1))
    mixing = jax.random.uniform(rate_key, (GROUPS, STATE), jnp.float32)
    slow_rate = 5.0 / TOKENS * jnp.exp(mixing * jnp.log(5.0))
    fast_rate = 0.6 * jnp.exp(mixing * jnp.log(2.0))
    return -jnp.where(slow, slow_rate, fast_rate)


def level_of(own_key, extent, shards, low, high):
    level = 1.0
    for position, parts in shards:
        heights = jax.random.uniform(jax.random.fold_in(jax.random.fold_in(own_key, 6), position), (parts,), jnp.float32, low / len(shards), high / len(shards))
        level = level * jnp.repeat(jnp.exp(heights), extent[position] // parts).reshape((-1,) + (1,) * (len(extent) - 1 - position))
    return level


def normal_values(key, shape, scale, bound, cuts=(), dtype=jnp.bfloat16):
    loudness = level_of(key, shape, cuts, -0.22, 0.18) if cuts else 1.0
    entries = jax.random.normal(key, shape, jnp.float32) * scale * loudness
    return jnp.minimum(jnp.maximum(entries, -bound), bound).astype(dtype)


def setup_inputs(seed: int = 0) -> dict:
    key_list = jax.random.split(jax.random.key(seed), 16)
    return {
        "mixer_in": normal_values(key_list[0], (TOKENS, CH), 1.0, 6.0, ((0, 64), (1, 8))),
        "residual": normal_values(key_list[1], (TOKENS, D), 1.0, 6.0, ((0, 512),)),
        "decay_real": draw_decay_real(jax.random.fold_in(key_list[15], 71), 0),
        "decay_imag": jnp.clip(1.0 + 199.0 * jax.random.uniform(key_list[3], (GROUPS, STATE), jnp.float32) ** level_of(key_list[3], (GROUPS, STATE), ((0, 8),), -0.2, 0.2), 1.0, 200.0),
        "log_step": jnp.clip(-3.9 + 1.4000001 * jax.random.uniform(key_list[4], (GROUPS,), jnp.float32) ** level_of(key_list[4], (GROUPS,), ((0, 8),), -0.2, 0.2), -3.9, -2.5),
        "in_real": normal_values(key_list[5], (GROUPS, STATE, GROUP), (2 * GROUP) ** -0.5, 1.0, ((0, 8),), jnp.float32),
        "in_imag": normal_values(key_list[6], (GROUPS, STATE, GROUP), (2 * GROUP) ** -0.5, 1.0, ((0, 8),), jnp.float32),
        "output_real": normal_values(key_list[7], (GROUPS, GROUP, STATE), (2 * STATE) ** -0.5, 0.5, ((0, 8),), jnp.float32),
        "output_imaginary": normal_values(key_list[8], (GROUPS, GROUP, STATE), (2 * STATE) ** -0.5, 0.5, ((0, 8),), jnp.float32),
        "skip": normal_values(key_list[9], (CH,), 1.0, 4.0, ((0, 8),), jnp.float32),
        "out_proj": normal_values(key_list[10], (CH, D), CH ** -0.5, 0.1875, ((0, 8),)),
        "norm_gain": jnp.clip(1.0 + 0.18 * jax.random.normal(key_list[11], (D,), jnp.float32), 0.1, 1.9),
        "w_gate": normal_values(key_list[12], (D, FF), D ** -0.5, 0.125, ((0, 64), (1, 8))),
        "w_up": normal_values(key_list[13], (D, FF), D ** -0.5, 0.125, ((0, 64), (1, 8))),
        "w_down": normal_values(key_list[14], (FF, D), FF ** -0.5, 0.078125, ((0, 8), (1, 64))),
    }


def discrete(decay_real, decay_imag, log_step, in_real, in_imag):
    step_size = jnp.exp(log_step)[:, None]
    magnitude = jnp.exp(decay_real * step_size)
    angle = decay_imag * step_size
    power_re = magnitude * jnp.cos(angle)
    power_im = magnitude * jnp.sin(angle)
    denom = decay_real * decay_real + decay_imag * decay_imag
    ratio_re = ((power_re - 1.0) * decay_real + power_im * decay_imag) / denom
    ratio_im = (power_im * decay_real - (power_re - 1.0) * decay_imag) / denom
    drive_re = ratio_re[..., None] * in_real - ratio_im[..., None] * in_imag
    drive_im = ratio_re[..., None] * in_imag + ratio_im[..., None] * in_real
    return (power_re, power_im, drive_re, drive_im)

def combine(earlier, later):
    ar1, ai1, br1, bi1 = earlier
    ar2, ai2, br2, bi2 = later
    return (ar2 * ar1 - ai2 * ai1, ar2 * ai1 + ai2 * ar1, ar2 * br1 - ai2 * bi1 + br2, ar2 * bi1 + ai2 * br1 + bi2)

def block_sum(left, right, width):
    summed = jnp.zeros((left.shape[0], right.shape[1]), jnp.float32)
    for index in range(left.shape[1] // width):
        partial_value = jnp.dot(left[:, index * width:(index + 1) * width], right[index * width:(index + 1) * width], preferred_element_type=jnp.float32).astype(jnp.bfloat16)
        summed = summed + lax.optimization_barrier(partial_value).astype(jnp.float32)
    return summed.astype(jnp.bfloat16)

def reference(mixer_in, residual, decay_real, decay_imag, log_step, in_real, in_imag, output_real, output_imaginary, skip, out_proj, norm_gain, w_gate, w_up, w_down):
    highest_precision = lax.Precision.HIGHEST
    power_re, power_im, bar_re, bar_im = discrete(decay_real, decay_imag, log_step, in_real, in_imag)
    groups, states = decay_real.shape
    signal = mixer_in.astype(jnp.float32).reshape(N_SP, TOK_DEV, groups, GROUP)
    group_skip_gain = skip.reshape(groups, GROUP)

    def advance(carry, block_range):
        hold_re, hold_im = carry
        drive_re = jnp.einsum('tgc,gpc->tgp', block_range, bar_re, precision=highest_precision)
        drive_im = jnp.einsum('tgc,gpc->tgp', block_range, bar_im, precision=highest_precision)
        a_re = jnp.broadcast_to(power_re[None], drive_re.shape)
        a_im = jnp.broadcast_to(power_im[None], drive_re.shape)
        pw_re, pw_im, state_real, state_imaginary = lax.associative_scan(combine, (a_re, a_im, drive_re, drive_im), axis=0)
        state_real = state_real + pw_re * hold_re[None] - pw_im * hold_im[None]
        state_imaginary = state_imaginary + pw_re * hold_im[None] + pw_im * hold_re[None]
        mixed_before_norm = jnp.einsum('uzl,zhl->uzh', state_real, output_real, precision=highest_precision) - jnp.einsum('uzl,zhl->uzh', state_imaginary, output_imaginary, precision=highest_precision) + group_skip_gain[None] * block_range
        return ((state_real[-1], state_imaginary[-1]), mixed_before_norm.reshape(TOK_DEV, groups * GROUP))
    zero_state = jnp.zeros((groups, states), jnp.float32)
    _, mixed_all = lax.scan(advance, (zero_state, zero_state), signal)
    activated = jax.nn.gelu(mixed_all).astype(jnp.bfloat16)
    res_blocks = residual.reshape(N_SP, TOK_DEV, residual.shape[1])

    def finish(pair):
        act_rows, res_rows = pair
        mixed = block_sum(act_rows, out_proj, CH_DEV)
        carried = res_rows.astype(jnp.float32) + mixed.astype(jnp.float32)
        scale = lax.rsqrt(lax.optimization_barrier(jnp.mean(carried * carried, axis=-1, keepdims=True)) + 1e-06)
        normed = (carried * scale * norm_gain).astype(jnp.bfloat16)
        gate = jnp.dot(normed, w_gate, preferred_element_type=jnp.float32)
        up = jnp.dot(normed, w_up, preferred_element_type=jnp.float32)
        hidden = (jax.nn.silu(gate) * up).astype(jnp.bfloat16)
        down = block_sum(hidden, w_down, FF_DEV)
        return (carried + 0.5 * down.astype(jnp.float32)).astype(jnp.bfloat16)
    result = lax.map(finish, (activated, res_blocks))
    return result.reshape(TOKENS, residual.shape[1])
```

```python
import functools

import jax
import jax.numpy as jnp
from jax import lax
from jax.experimental import pallas as pl
from jax.experimental.pallas import tpu as pltpu
from jax.sharding import Mesh
from jax.sharding import PartitionSpec as P

SP = ("sp_0", "sp_1")
SP_TP = ("sp_0", "sp_1", "tp")
MESH = pl.DeviceIdType.MESH
F32 = jnp.float32
BF16 = jnp.bfloat16

NZ = 16
NY = 4
NX = 4
NT = 8
HALF = NZ // 2
D = 2048
TOK = 512
ROWS = TOK // NT
FL = 512
CHD = 128
FFD = 704
KB = 32
GU = 2 * FFD
Q = 176


def discrete(decay_real, decay_imag, log_step):
    step_size = jnp.exp(log_step)[:, None]
    magnitude = jnp.exp(decay_real * step_size)
    angle = decay_imag * step_size
    power_re = magnitude * jnp.cos(angle)
    power_im = magnitude * jnp.sin(angle)
    denom = decay_real * decay_real + decay_imag * decay_imag
    ratio_re = ((power_re - 1.0) * decay_real + power_im * decay_imag) / denom
    ratio_im = (power_im * decay_real - (power_re - 1.0) * decay_imag) / denom
    return jnp.stack([power_re, power_im, ratio_re, ratio_im])


def cmul(a, b):
    return (a[0] * b[0] - a[1] * b[1], a[0] * b[1] + a[1] * b[0])


def cadd(a, b):
    return (a[0] + b[0], a[1] + b[1])


def pieces(v):
    hi = v.astype(BF16)
    lo = (v - hi.astype(F32)).astype(BF16)
    return hi, lo


def dot(a, b):
    return jnp.dot(a, b, preferred_element_type=F32)


def dot_t(a, b):
    return lax.dot_general(a, b, (((1,), (1,)), ((), ())), preferred_element_type=F32)


def packed(row):
    return jnp.concatenate([row[:, i * 128 : (i + 1) * 128] for i in range(4)], axis=0)


def flat(block):
    return jnp.concatenate([block[i : i + 1] for i in range(4)], axis=1)


def kernel(
    x_ref, cf_ref, inr_ref, ini_ref, our_ref, oui_ref, skip_ref, op_ref, gain_ref,
    res_ref, wg_ref, wu_ref, wd_ref, out_ref,
    wgu, wdn, dy, opall, sb, tb, act, acts, nf, hid, part, pr, ps, rs1, rs2, rs3,
    ur, ui, mr, mi, er, ei, pcr, pci, carried,
    g_recv, gz_send, gy_send, d_recv, dz_send, dy_recv, dy_send,
    o_recv, o_send, s_recv, s_send, t_recv, t_send, a_recv, a_send,
    n_recv, n_send, p_recv, p_send, r_recv, r_send,
):
    z = lax.axis_index("sp_0")
    y = lax.axis_index("sp_1")
    t = lax.axis_index("tp")
    x = t // 2
    c = t % 2
    yp = (y + 1 + 2 * c) % NY
    ym = (y + 3 + 2 * c) % NY
    y2 = (y + 2) % NY
    zp = (z + 1 + (NZ - 2) * c) % NZ
    zm = (z + NZ - 1 + 2 * c) % NZ
    xp = (x + 1 + 2 * c) % NX
    xm = (x + 3 + 2 * c) % NX
    x2 = (x + 2) % NX
    other = 1 - c
    tpp = xp * 2 + c
    tpm = xm * 2 + c
    tp2 = x2 * 2 + c
    tpo = x * 2 + other
    sent = []

    def copy(src, dst, ss, rs, **dev):
        return pltpu.make_async_remote_copy(
            src_ref=src, dst_ref=dst, send_sem=ss, recv_sem=rs, device_id=dev, device_id_type=MESH
        )

    def send(src, dst, ss, rs, **dev):
        cp = copy(src, dst, ss, rs, **dev)
        cp.start()
        sent.append(cp)

    def arrived(dst, ss, rs, **dev):
        copy(dst, dst, ss, rs, **dev).wait_recv()

    barrier = pltpu.get_barrier_semaphore()
    for k in range(1, NT):
        pl.semaphore_signal(barrier, inc=1, device_id={"tp": (t + k) % NT}, device_id_type=MESH)
    for k in range(1, NY):
        pl.semaphore_signal(barrier, inc=1, device_id={"sp_1": (y + k) % NY}, device_id_type=MESH)
    for k in range(1, NZ):
        pl.semaphore_signal(barrier, inc=1, device_id={"sp_0": (z + k) % NZ}, device_id_type=MESH)

    own = z * NY + y
    wgu[own, :, 0:640] = wg_ref[:, 0:640]
    wgu[own, :, 640:1280] = wu_ref[:, 0:640]
    wgu[own, :, 1280:1408] = jnp.concatenate([wg_ref[:, 640:704], wu_ref[:, 640:704]], axis=1)
    dy[y] = jnp.concatenate([wd_ref[q * Q : (q + 1) * Q] for q in range(4)], axis=1)
    opall[t] = op_ref[...]

    pl.semaphore_wait(barrier, NT - 1 + NY - 1 + NZ - 1)

    def g_blk(zb, yb):
        return wgu.at[zb * NY + yb]

    def g_z_forward(zb, chain, s):
        blk = g_blk(zb, y)
        send(blk, blk, gz_send.at[chain * HALF + s], g_recv.at[zb * NY + y],
             sp_0=zp if chain == 0 else zm)

    def g_y_start(zb, o):
        blk = g_blk(zb, y)
        send(blk, blk, gy_send.at[3 * o], g_recv.at[zb * NY + y], sp_1=yp)
        send(blk, blk, gy_send.at[3 * o + 1], g_recv.at[zb * NY + y], sp_1=ym)

    def g_y_forward(zb, o):
        blk = g_blk(zb, ym)
        arrived(blk, gy_send.at[3 * o + 2], g_recv.at[zb * NY + ym], sp_1=ym)
        send(blk, blk, gy_send.at[3 * o + 2], g_recv.at[zb * NY + ym], sp_1=yp)

    def g_y_finish(zb, o):
        for yb in (yp, y2):
            arrived(g_blk(zb, yb), gy_send.at[3 * o], g_recv.at[zb * NY + yb], sp_1=yp)

    def chain_block(chain, s):
        toward = zm - z if chain == 0 else zp - z
        return (z + NZ * NZ + s * toward) % NZ

    def d_z_forward(zb, chain, s):
        send(wdn.at[zb], wdn.at[zb], dz_send.at[chain * HALF + s], d_recv.at[zb],
             sp_0=zp if chain == 0 else zm)

    def d_start():
        for k in range(1, NY):
            yk = (y + k) % NY
            arrived(dy.at[yk], dy_send.at[k], dy_recv.at[yk], sp_1=yk)
        for q in range(4):
            wdn[z, q * Q : (q + 1) * Q, :] = jnp.concatenate(
                [dy[b, :, q * KB : (q + 1) * KB] for b in range(NY)], axis=1
            )
        d_z_forward(z, 0, 0)
        d_z_forward(z, 1, 0)

    def steps(s):
        return [(0, s)] + ([(1, s)] if s < HALF else [])

    def order(chain, s):
        return 0 if s == 0 else 2 * s - 1 + chain

    def tick(s):
        for chain, s_ in steps(s):
            zb = chain_block(chain, s_)
            arrived(g_blk(zb, y), gz_send.at[0], g_recv.at[zb * NY + y], sp_0=zm)
            if s_ < (HALF if chain == 0 else HALF - 1):
                g_z_forward(zb, chain, s_)
            g_y_start(zb, order(chain, s_))
        if s == 1:
            g_y_forward(z, 0)
        else:
            for chain, s_ in steps(s - 1):
                g_y_forward(chain_block(chain, s_), order(chain, s_))
        for chain, s_ in steps(s):
            zb = chain_block(chain, s_)
            arrived(wdn.at[zb], dz_send.at[0], d_recv.at[zb], sp_0=zm)
            if s_ < (HALF if chain == 0 else HALF - 1):
                d_z_forward(zb, chain, s_)

    def tp_start(buf, recv, ssem):
        send(buf.at[t], buf.at[t], ssem.at[0], recv.at[t], tp=tpp)
        send(buf.at[t], buf.at[t], ssem.at[1], recv.at[t], tp=tpm)
        send(buf.at[t], buf.at[t], ssem.at[2], recv.at[t], tp=tpo)

    def tp_forward(buf, recv, ssem):
        arrived(buf.at[tpm], ssem.at[0], recv.at[tpm], tp=tpm)
        send(buf.at[tpm], buf.at[tpm], ssem.at[3], recv.at[tpm], tp=tpp)
        send(buf.at[tpm], buf.at[tpm], ssem.at[4], recv.at[tpm], tp=tpo)
        arrived(buf.at[tpp], ssem.at[0], recv.at[tpp], tp=tpp)
        send(buf.at[tpp], buf.at[tpp], ssem.at[5], recv.at[tpp], tp=tpo)

    def tp_last(buf, recv, ssem):
        arrived(buf.at[tp2], ssem.at[0], recv.at[tp2], tp=tpm)
        send(buf.at[tp2], buf.at[tp2], ssem.at[6], recv.at[tp2], tp=tpo)

    def tp_finish(buf, recv, ssem):
        for xb in (x, xp, xm, x2):
            b = xb * 2 + other
            arrived(buf.at[b], ssem.at[0], recv.at[b], tp=tpo)

    for k in range(1, NY):
        yk = (y + k) % NY
        send(dy.at[y], dy.at[y], dy_send.at[k], dy_recv.at[y], sp_1=yk)
    g_z_forward(z, 0, 0)
    g_z_forward(z, 1, 0)
    g_y_start(z, 0)
    tp_start(opall, o_recv, o_send)

    a = (cf_ref[0:1], cf_ref[1:2])
    ratio = (cf_ref[2:3], cf_ref[3:4])
    powers = [a]
    for _ in range(7):
        powers.append(cmul(powers[-1], a))
    lift = tuple(jnp.concatenate([p[i] for p in powers], axis=0) for i in (0, 1))
    row8 = lax.broadcasted_iota(jnp.int32, (8, FL), 0)
    masked = []
    for k in (1, 2, 4):
        p = powers[k - 1]
        masked.append(tuple(jnp.where(row8 >= k, jnp.broadcast_to(v, (8, FL)), 0.0) for v in p))

    spread = (
        lax.broadcasted_iota(jnp.int32, (16, CHD), 1) % 16
        == lax.broadcasted_iota(jnp.int32, (16, CHD), 0)
    ).astype(F32).astype(BF16)
    block = (
        lax.broadcasted_iota(jnp.int32, (FL, CHD), 0) // 64
        == lax.broadcasted_iota(jnp.int32, (FL, CHD), 1) // 16
    )
    signal = x_ref[...]
    for src, dst in ((inr_ref, ur), (ini_ref, ui)):
        total = None
        for piece in pieces(src[...]):
            wide = jnp.where(block, dot(piece, spread), 0.0).astype(BF16)
            term = dot_t(signal, wide)
            total = term if total is None else total + term
        dst[...] = total

    def tile_step(i, carry):
        for j in range(4):
            rows = pl.ds(pl.multiple_of(i * 32 + j * 8, 8), 8)
            v = cmul(ratio, (ur[rows, :], ui[rows, :]))
            for k, m in zip((1, 2, 4), masked):
                v = cadd(v, cmul(m, (pltpu.roll(v[0], k, 0), pltpu.roll(v[1], k, 0))))
            ur[rows, :] = v[0]
            ui[rows, :] = v[1]
            er[pl.ds(i * 4 + j, 1), :] = v[0][7:8]
            ei[pl.ds(i * 4 + j, 1), :] = v[1][7:8]
        return carry

    lax.fori_loop(0, TOK // 32, tile_step, 0)

    row64 = lax.broadcasted_iota(jnp.int32, (64, FL), 0)
    e = (er[...], ei[...])
    ladder = []
    p = powers[7]
    for k in (1, 2, 4, 8, 16, 32):
        ladder.append(p)
        moved = tuple(jnp.where(row64 >= k, pltpu.roll(v, k, 0), 0.0) for v in e)
        e = cadd(e, cmul(p, moved))
        p = cmul(p, p)
    er[...] = e[0]
    ei[...] = e[1]
    a512 = (packed(p[0]), packed(p[1]))
    last = (e[0][63:64], e[1][63:64])
    sb[y, 0:4, :] = packed(last[0])
    sb[y, 4:8, :] = packed(last[1])
    for k in range(1, NY):
        send(sb.at[y], sb.at[y], s_send.at[k], s_recv.at[y], sp_1=(y + k) % NY)

    d_start()

    lead = (jnp.ones((64, FL), F32), jnp.zeros((64, FL), F32))
    for b, q in enumerate(ladder):
        more = cmul(q, lead)
        bit = (row64 // (1 << b)) % 2 == 1
        lead = tuple(jnp.where(bit, m, v) for m, v in zip(more, lead))
    pcr[...] = lead[0]
    pci[...] = lead[1]

    for k in range(1, NY):
        yk = (y + k) % NY
        arrived(sb.at[yk], s_send.at[k], s_recv.at[yk], sp_1=yk)
    whole = (jnp.zeros((4, 128), F32), jnp.zeros((4, 128), F32))
    before = whole
    ahead = (jnp.ones((4, 128), F32), jnp.zeros((4, 128), F32))
    for b in range(NY):
        own_b = (sb[b, 0:4, :], sb[b, 4:8, :])
        whole = cadd(cmul(a512, whole), own_b)
        inside = b < y
        step_b = cadd(cmul(a512, before), own_b)
        before = tuple(jnp.where(inside, n, v) for n, v in zip(step_b, before))
        step_a = cmul(a512, ahead)
        ahead = tuple(jnp.where(inside, n, v) for n, v in zip(step_a, ahead))
    a2 = cmul(a512, a512)
    a4 = cmul(a2, a2)
    tb[z, 0:4, :] = whole[0]
    tb[z, 4:8, :] = whole[1]
    for k in range(1, NZ):
        send(tb.at[z], tb.at[z], t_send.at[k], t_recv.at[z], sp_0=(z + k) % NZ)

    spread2 = (
        lax.broadcasted_iota(jnp.int32, (64, FL), 1) % 64
        == lax.broadcasted_iota(jnp.int32, (64, FL), 0)
    ).astype(F32).astype(BF16)
    block2 = (
        lax.broadcasted_iota(jnp.int32, (CHD, FL), 0) // 16
        == lax.broadcasted_iota(jnp.int32, (CHD, FL), 1) // 64
    )
    for k, (src, sign) in enumerate(((our_ref, 1.0), (oui_ref, -1.0))):
        hi, lo = pieces(src[...] * sign)
        mr[k] = jnp.where(block2, dot(hi, spread2), 0.0).astype(BF16)
        mi[k] = jnp.where(block2, dot(lo, spread2), 0.0).astype(BF16)

    tick(1)

    for k in range(1, NZ):
        zk = (z + k) % NZ
        arrived(tb.at[zk], t_send.at[k], t_recv.at[zk], sp_0=zk)
    hold = (jnp.zeros((4, 128), F32), jnp.zeros((4, 128), F32))
    for b in range(NZ - 1):
        step_h = cadd(cmul(a4, hold), (tb[b, 0:4, :], tb[b, 4:8, :]))
        hold = tuple(jnp.where(b < z, n, v) for n, v in zip(step_h, hold))
    hold = cadd(cmul(ahead, hold), before)
    hold = (flat(hold[0]), flat(hold[1]))
    enter = cmul((pcr[...], pci[...]), hold)
    prev = tuple(jnp.where(row64 >= 1, pltpu.roll(v[...], 1, 0), 0.0) for v in (er, ei))
    enter = cadd(enter, prev)
    pcr[...] = enter[0]
    pci[...] = enter[1]

    def read_step(i, carry):
        re, im = [], []
        for j in range(16):
            k = i * 16 + j
            rows = pl.ds(pl.multiple_of(k * 8, 8), 8)
            w = (pcr[pl.ds(k, 1), :], pci[pl.ds(k, 1), :])
            v = cadd((ur[rows, :], ui[rows, :]), cmul(lift, w))
            re.append(v[0])
            im.append(v[1])
        total = None
        for k, v in enumerate((re, im)):
            hi, lo = pieces(jnp.concatenate(v, axis=0))
            term = dot_t(hi, mr[k]) + dot_t(hi, mi[k]) + dot_t(lo, mr[k])
            total = term if total is None else total + term
        rows = pl.ds(pl.multiple_of(i * 128, 128), 128)
        pre = total + skip_ref[...] * x_ref[rows, :].astype(F32)
        inner = 0.7978845608028654 * (pre + 0.044715 * (pre * pre * pre))
        val = (pre * (0.5 * (1.0 + jnp.tanh(inner)))).astype(BF16)
        act[2 * i] = val[0:64]
        act[2 * i + 1] = val[64:128]
        return carry

    lax.fori_loop(0, 4, read_step, 0)
    for k in range(1, NT):
        tk = (t + k) % NT
        send(act.at[tk], acts.at[t], a_send.at[k], a_recv.at[t], tp=tk)
    acts[t] = act[t]

    tp_forward(opall, o_recv, o_send)
    tick(2)
    tp_last(opall, o_recv, o_send)
    tp_finish(opall, o_recv, o_send)

    for k in range(1, NT):
        tk = (t + k) % NT
        arrived(acts.at[tk], a_send.at[k], a_recv.at[tk], tp=tk)

    def mix_step(j, squares):
        cols = pl.ds(pl.multiple_of(j * 256, 256), 256)
        total = jnp.zeros((ROWS, 256), F32)
        for b in range(NT):
            total = total + dot(acts[b], opall[b, :, cols]).astype(BF16).astype(F32)
        v = res_ref[:, cols].astype(F32) + total.astype(BF16).astype(F32)
        carried[:, cols] = v
        return squares + jnp.sum(v * v, axis=1, keepdims=True)

    squares = lax.fori_loop(0, D // 256, mix_step, jnp.zeros((ROWS, 1), F32))
    scale = lax.rsqrt(squares * (1.0 / D) + 1e-06)
    nf[t] = (carried[...] * scale * gain_ref[...]).astype(BF16)
    tp_start(nf, n_recv, n_send)
    tick(3)
    tp_forward(nf, n_recv, n_send)
    tick(4)
    tp_last(nf, n_recv, n_send)
    tp_finish(nf, n_recv, n_send)
    for s in range(5, HALF + 1):
        tick(s)
    for chain, s_ in steps(HALF):
        g_y_forward(chain_block(chain, s_), order(chain, s_))
    g_y_finish(z, 0)
    for s in range(1, HALF + 1):
        for chain, s_ in steps(s):
            g_y_finish(chain_block(chain, s_), order(chain, s_))

    def up_step(j, carry):
        c0 = pl.ds(pl.multiple_of(j * 128, 128), 128)
        c1 = pl.ds(pl.multiple_of(640 + j * 128, 128), 128)
        w = jnp.concatenate(
            [wgu[:, :, c0].reshape(D, 128), wgu[:, :, c1].reshape(D, 128)], axis=1
        )
        v = dot(nf[...].reshape(TOK, D), w)
        g = v[:, 0:128]
        hid[:, c0] = (g / (1.0 + jnp.exp(-g)) * v[:, 128:256]).astype(BF16)
        return carry

    lax.fori_loop(0, 5, up_step, 0)
    v = dot(nf[...].reshape(TOK, D), wgu[:, :, 1280:1408].reshape(D, 128))
    tail = v / (1.0 + jnp.exp(-v)) * pltpu.roll(v, 64, 1)
    hid[:, 640:704] = tail[:, 0:64].astype(BF16)

    def down_step(j, carry):
        w = jnp.concatenate([wdn[2 * j], wdn[2 * j + 1]], axis=1)
        cols = pl.ds(pl.multiple_of(j * 256, 256), 256)
        part[:, :, cols] = dot(hid[...], w).astype(BF16).reshape(NT, ROWS, 256)
        return carry

    lax.fori_loop(0, NZ // 2, down_step, 0)

    targets = (x2, xm, xp, x)
    for k, xb in enumerate(targets):
        send(part.at[xb * 2 + other], pr.at[xb], p_send.at[k], p_recv.at[xb], tp=tpo)

    def pair(xb):
        arrived(pr.at[xb], p_send.at[0], p_recv.at[xb], tp=tpo)
        return part[xb * 2 + c].astype(F32) + pr[xb].astype(F32)

    ps[0] = pair(x2).astype(BF16)
    send(ps.at[0], rs1, r_send.at[0], r_recv.at[0], tp=tpp)
    ps[1] = pair(xm).astype(BF16)
    send(ps.at[1], rs2, r_send.at[1], r_recv.at[1], tp=tpm)
    near = pair(xp)
    arrived(rs1, r_send.at[0], r_recv.at[0], tp=tpm)
    ps[2] = (near + rs1[...].astype(F32)).astype(BF16)
    send(ps.at[2], rs3, r_send.at[2], r_recv.at[2], tp=tpp)
    mine = pair(x)
    arrived(rs2, r_send.at[1], r_recv.at[1], tp=tpp)
    arrived(rs3, r_send.at[2], r_recv.at[2], tp=tpm)
    down = (mine + rs2[...].astype(F32) + rs3[...].astype(F32)).astype(BF16)
    out_ref[...] = (carried[...] + 0.5 * down.astype(F32)).astype(BF16)

    for cp in sent:
        cp.wait_send()


def on_device(
    mixer_in, residual, decay_real, decay_imag, log_step, in_real, in_imag,
    output_real, output_imaginary, skip, out_proj, norm_gain, w_gate, w_up, w_down,
):
    cf = discrete(decay_real, decay_imag, log_step).reshape(4, FL)
    vmem = pltpu.VMEM
    dma = pltpu.SemaphoreType.DMA
    scratch = [
        vmem((NZ * NY, KB, GU), BF16),
        vmem((NZ, FFD, 128), BF16),
        vmem((NY, Q, 128), BF16),
        vmem((NT, CHD, D), BF16),
        vmem((NY, 8, 128), F32),
        vmem((NZ, 8, 128), F32),
        vmem((NT, ROWS, CHD), BF16),
        vmem((NT, ROWS, CHD), BF16),
        vmem((NT, ROWS, D), BF16),
        vmem((TOK, FFD), BF16),
        vmem((NT, ROWS, D), BF16),
        vmem((NX, ROWS, D), BF16),
        vmem((3, ROWS, D), BF16),
        vmem((ROWS, D), BF16),
        vmem((ROWS, D), BF16),
        vmem((ROWS, D), BF16),
        vmem((TOK, FL), F32),
        vmem((TOK, FL), F32),
        vmem((2, CHD, FL), BF16),
        vmem((2, CHD, FL), BF16),
        vmem((64, FL), F32),
        vmem((64, FL), F32),
        vmem((64, FL), F32),
        vmem((64, FL), F32),
        vmem((ROWS, D), F32),
        dma((NZ * NY,)), dma((NZ,)), dma((3 * NZ,)), dma((NZ,)), dma((NZ,)),
        dma((NY,)), dma((NY,)),
        dma((NT,)), dma((7,)), dma((NY,)), dma((NY,)), dma((NZ,)), dma((NZ,)),
        dma((NT,)), dma((NT,)), dma((NT,)), dma((7,)), dma((NX,)), dma((NX,)),
        dma((3,)), dma((3,)),
    ]
    return pl.pallas_call(
        kernel,
        out_shape=jax.ShapeDtypeStruct((ROWS, D), BF16),
        in_specs=[pl.BlockSpec(memory_space=vmem)] * 13,
        out_specs=pl.BlockSpec(memory_space=vmem),
        scratch_shapes=scratch,
        compiler_params=pltpu.CompilerParams(
            collective_id=0, has_side_effects=True, vmem_limit_bytes=60 * 1024 * 1024
        ),
    )(
        mixer_in, cf, in_real.reshape(FL, 16), in_imag.reshape(FL, 16),
        output_real.reshape(CHD, 64), output_imaginary.reshape(CHD, 64),
        skip.reshape(1, CHD), out_proj, norm_gain.reshape(1, D),
        residual, w_gate, w_up, w_down,
    )


def solution(mesh):
    finer = Mesh(mesh.devices.reshape(NZ, NY, mesh.shape["tp"]), ("sp_0", "sp_1", "tp"))
    return jax.shard_map(
        on_device,
        mesh=finer,
        in_specs=(
            P(SP, "tp"),
            P(SP_TP, None),
            P("tp", None),
            P("tp", None),
            P("tp"),
            P("tp", None, None),
            P("tp", None, None),
            P("tp", None, None),
            P("tp", None, None),
            P("tp"),
            P("tp", None),
            P(),
            P(SP, "tp"),
            P(SP, "tp"),
            P("tp", SP),
        ),
        out_specs=P(SP_TP, None),
        check_vma=False,
    )
```

```python
import functools

import jax
import jax.numpy as jnp
from jax import lax
from jax.experimental import pallas as pl
from jax.experimental.pallas import tpu as pltpu
from jax.sharding import Mesh
from jax.sharding import PartitionSpec as P

SP = ("sp_0", "sp_1")
SP_TP = ("sp_0", "sp_1", "tp")
MESH = pl.DeviceIdType.MESH
F32 = jnp.float32
BF16 = jnp.bfloat16

NZ = 16
NY = 4
NX = 4
NT = 8
HALF = NZ // 2
D = 2048
TOK = 512
ROWS = TOK // NT
FL = 512
CHD = 128
FFD = 704
GU = 2 * FFD
CA = 512
SPANS = ((0, 3), (3, 6), (6, 7), (7, 8))
NC = len(SPANS)


def discrete(decay_real, decay_imag, log_step):
    step_size = jnp.exp(log_step)
    magnitude = jnp.exp(decay_real * step_size)
    angle = decay_imag * step_size
    power_re = magnitude * jnp.cos(angle)
    power_im = magnitude * jnp.sin(angle)
    denom = decay_real * decay_real + decay_imag * decay_imag
    ratio_re = ((power_re - 1.0) * decay_real + power_im * decay_imag) / denom
    ratio_im = (power_im * decay_real - (power_re - 1.0) * decay_imag) / denom
    return (power_re, power_im), (ratio_re, ratio_im)


def cmul(a, b):
    return (a[0] * b[0] - a[1] * b[1], a[0] * b[1] + a[1] * b[0])


def cadd(a, b):
    return (a[0] + b[0], a[1] + b[1])


def pieces(v):
    hi = v.astype(BF16)
    lo = (v - hi.astype(F32)).astype(BF16)
    return hi, lo


def dot(a, b):
    return jnp.dot(a, b, preferred_element_type=F32)


def dot_t(a, b):
    return lax.dot_general(a, b, (((1,), (1,)), ((), ())), preferred_element_type=F32)


def packed(row):
    return jnp.concatenate([row[:, i * 128 : (i + 1) * 128] for i in range(4)], axis=0)


def flat(block):
    return jnp.concatenate([block[i : i + 1] for i in range(4)], axis=1)


class Phase:
    def __init__(self):
        self.scope = None

    def __call__(self, name):
        if self.scope is not None:
            self.scope.__exit__(None, None, None)
        self.scope = None
        if name:
            self.scope = jax.named_scope(name)
            self.scope.__enter__()


class Ring:
    count = 33

    def __init__(self, net, buf, sems):
        self.net, self.buf = net, buf
        (self.ya_recv, self.ya_send, self.za_recv, self.za_send,
         self.zb_recv, self.zb_send, self.yb_recv, self.yb_send) = sems

    def a_y(self, zb, yb):
        return self.buf.at[zb * NY + yb, :, 0:CA]

    def a_z(self, zb, h):
        return self.buf.at[pl.ds(zb * NY + 2 * h, 2), :, 0:CA]

    def b(self, zb, yb):
        return self.buf.at[zb * NY + yb, :, CA:GU]

    def start_ya(self):
        n = self.net
        blk = self.a_y(n.z, n.y)
        for k in range(1, NY):
            n.send(blk, blk, self.ya_send.at[k], self.ya_recv.at[n.y], sp_1=(n.y + k) % NY)

    def finish_ya(self):
        n = self.net
        for k in range(1, NY):
            yk = (n.y + k) % NY
            n.arrived(self.a_y(n.z, yk), self.ya_send.at[k], self.ya_recv.at[yk], sp_1=yk)

    def forward_a(self, zb, chain, s, h):
        n = self.net
        blk = self.a_z(zb, h)
        n.send(blk, blk, self.za_send.at[(chain * HALF + s) * 2 + h], self.za_recv.at[zb * 2 + h],
               sp_0=n.zp if chain == 0 else n.zm)

    def forward_b(self, zb, chain, s):
        n = self.net
        blk = self.b(zb, n.y)
        n.send(blk, blk, self.zb_send.at[chain * HALF + s], self.zb_recv.at[zb],
               sp_0=n.zp if chain == 0 else n.zm)

    def start_yb(self, zb, o):
        n = self.net
        blk = self.b(zb, n.y)
        sem = self.yb_recv.at[zb * NY + n.y]
        n.send(blk, blk, self.yb_send.at[3 * o], sem, sp_1=n.yp)
        n.send(blk, blk, self.yb_send.at[3 * o + 1], sem, sp_1=n.ym)

    def own_a(self):
        self.finish_ya()
        for h in (0, 1):
            for chain in (0, 1):
                self.forward_a(self.net.z, chain, 0, h)

    def own_bz(self):
        for chain in (0, 1):
            self.forward_b(self.net.z, chain, 0)

    def own_by(self):
        self.start_yb(self.net.z, 0)

    def tick_a(self, s, h):
        n = self.net
        for chain in n.chains(s):
            zb = n.block(chain, s)
            n.arrived(self.a_z(zb, h), self.za_send.at[0], self.za_recv.at[zb * 2 + h], sp_0=n.zm)
            if n.goes_on(chain, s):
                self.forward_a(zb, chain, s, h)

    def tick_b(self, s):
        n = self.net
        for chain in n.chains(s):
            zb = n.block(chain, s)
            n.arrived(self.b(zb, n.y), self.zb_send.at[0], self.zb_recv.at[zb], sp_0=n.zm)
            if n.goes_on(chain, s):
                self.forward_b(zb, chain, s)
            self.start_yb(zb, n.order(chain, s))

    def tick_y(self, s):
        n = self.net
        for chain in n.chains(s):
            zb, o = n.block(chain, s), n.order(chain, s)
            blk = self.b(zb, n.ym)
            sem = self.yb_recv.at[zb * NY + n.ym]
            n.arrived(blk, self.yb_send.at[3 * o + 2], sem, sp_1=n.ym)
            n.send(blk, blk, self.yb_send.at[3 * o + 2], sem, sp_1=n.yp)

    def finish(self, s):
        n = self.net
        for chain in n.chains(s):
            zb, o = n.block(chain, s), n.order(chain, s)
            for yb in (n.yp, n.y2):
                n.arrived(self.b(zb, yb), self.yb_send.at[3 * o],
                          self.yb_recv.at[zb * NY + yb], sp_1=n.yp)


RING_SEMS = [NY, NY, 2 * NZ, 4 * HALF, NZ, NZ, NZ * NY, 3 * NZ]


class Pool:
    def __init__(self, net, buf, recv, ssem):
        self.net, self.buf, self.recv, self.ssem = net, buf, recv, ssem

    def at(self, b, h):
        return self.buf.at[b, :, h * (D // 2) : (h + 1) * (D // 2)]

    def put(self, b, h, k, to):
        blk = self.at(b, h)
        self.net.send(blk, blk, self.ssem.at[2 * k + h], self.recv.at[b * 2 + h], tp=to)

    def get(self, b, h, frm):
        self.net.arrived(self.at(b, h), self.ssem.at[0], self.recv.at[b * 2 + h], tp=frm)

    def start(self, h):
        n = self.net
        self.put(n.t, h, 0, n.tpp)
        self.put(n.t, h, 1, n.tpm)
        self.put(n.t, h, 2, n.tpo)

    def forward(self, h):
        n = self.net
        self.get(n.tpm, h, n.tpm)
        self.put(n.tpm, h, 3, n.tpp)
        self.put(n.tpm, h, 4, n.tpo)
        self.get(n.tpp, h, n.tpp)
        self.put(n.tpp, h, 5, n.tpo)

    def last(self, h):
        n = self.net
        self.get(n.tp2, h, n.tpm)
        self.put(n.tp2, h, 6, n.tpo)

    def finish(self, h):
        n = self.net
        for xb in (n.x, n.xp, n.xm, n.x2):
            self.get(xb * 2 + n.other, h, n.tpo)


class Net:
    def __init__(self):
        self.z = lax.axis_index("sp_0")
        self.y = lax.axis_index("sp_1")
        self.t = lax.axis_index("tp")
        z, y, t = self.z, self.y, self.t
        x, c = t // 2, t % 2
        self.x, self.c = x, c
        self.yp = (y + 1 + 2 * c) % NY
        self.ym = (y + 3 + 2 * c) % NY
        self.y2 = (y + 2) % NY
        self.zp = (z + 1 + (NZ - 2) * c) % NZ
        self.zm = (z + NZ - 1 + 2 * c) % NZ
        self.xp = (x + 1 + 2 * c) % NX
        self.xm = (x + 3 + 2 * c) % NX
        self.x2 = (x + 2) % NX
        self.other = 1 - c
        self.tpp = self.xp * 2 + c
        self.tpm = self.xm * 2 + c
        self.tp2 = self.x2 * 2 + c
        self.tpo = x * 2 + self.other
        self.sent = []

    def copy(self, src, dst, ss, rs, **dev):
        return pltpu.make_async_remote_copy(
            src_ref=src, dst_ref=dst, send_sem=ss, recv_sem=rs, device_id=dev, device_id_type=MESH
        )

    def send(self, src, dst, ss, rs, **dev):
        cp = self.copy(src, dst, ss, rs, **dev)
        cp.start()
        self.sent.append(cp)

    def arrived(self, dst, ss, rs, **dev):
        self.copy(dst, dst, ss, rs, **dev).wait_recv()

    def chains(self, s):
        return (0,) if s in (0, HALF) else (0, 1)

    def goes_on(self, chain, s):
        return s < (HALF if chain == 0 else HALF - 1)

    def block(self, chain, s):
        toward = self.zm - self.z if chain == 0 else self.zp - self.z
        return (self.z + NZ * NZ + s * toward) % NZ

    def order(self, chain, s):
        return 0 if s == 0 else 2 * s - 1 + chain


def kernel(
    x_ref, dr_ref, di_ref, ls_ref, inr_ref, ini_ref, our_ref, oui_ref, skip_ref, op_ref, gain_ref,
    res_ref, wg_ref, wu_ref, wd_ref, out_ref,
    wgu, wdn, opall, sb, tb, act, acts, nf, hid, part, pr, ps, rs,
    ur, ui, mr, mi, er, ei, pcr, pci, carried, *sems,
):
    net = Net()
    phase = Phase()
    z, y, t = net.z, net.y, net.t
    send, arrived = net.send, net.arrived
    gu = Ring(net, wgu, sems[0:8])
    dn = Ring(net, wdn, sems[8:16])
    (o_recv, o_send, n_recv, n_send, s_recv, s_send, t_recv, t_send, a_recv, a_send,
     p_recv, p_send, r_recv, r_send) = sems[16:]
    oproj = Pool(net, opall, o_recv, o_send)
    norms = Pool(net, nf, n_recv, n_send)

    phase("signal")
    barrier = pltpu.get_barrier_semaphore()
    for k in range(1, NZ):
        pl.semaphore_signal(barrier, inc=1, device_id={"sp_0": (z + k) % NZ}, device_id_type=MESH)
    for k in range(1, NY):
        pl.semaphore_signal(barrier, inc=1, device_id={"sp_1": (y + k) % NY}, device_id_type=MESH)
    for k in range(1, NT):
        pl.semaphore_signal(barrier, inc=1, device_id={"tp": (t + k) % NT}, device_id_type=MESH)

    phase("own")
    own = z * NY + y
    wgu[own, :, 0:640] = wg_ref[:, 0:640]
    wgu[own, :, 640:1280] = wu_ref[:, 0:640]
    wgu[own, :, 1280:1408] = jnp.concatenate([wg_ref[:, 640:704], wu_ref[:, 640:704]], axis=1)
    wdn[own, :, 0:640] = wd_ref[0:16, 0:640]
    wdn[own, :, 640:1280] = wd_ref[16:32, 0:640]
    wdn[own, :, 1280:1408] = jnp.concatenate([wd_ref[0:16, 640:704], wd_ref[16:32, 640:704]], axis=1)
    opall[t] = op_ref[...]

    phase("coef")
    eight = lax.broadcasted_iota(jnp.int32, (8, 8), 0) == lax.broadcasted_iota(jnp.int32, (8, 8), 1)
    log_step = jnp.sum(
        jnp.where(eight, jnp.broadcast_to(ls_ref[...], (8, 8)), 0.0), axis=1, keepdims=True
    )
    a, ratio = discrete(dr_ref[...], di_ref[...], log_step)

    def line(v):
        return jnp.concatenate([v[g : g + 1] for g in range(8)], axis=1)

    a = (line(a[0]), line(a[1]))
    ratio = (line(ratio[0]), line(ratio[1]))
    powers = [a]
    for _ in range(7):
        powers.append(cmul(powers[-1], a))
    lift = tuple(jnp.concatenate([p[i] for p in powers], axis=0) for i in (0, 1))
    row8 = lax.broadcasted_iota(jnp.int32, (8, FL), 0)
    masked = []
    for k in (1, 2, 4):
        p = powers[k - 1]
        masked.append(tuple(jnp.where(row8 >= k, jnp.broadcast_to(v, (8, FL)), 0.0) for v in p))

    phase("drive")
    spread = (
        lax.broadcasted_iota(jnp.int32, (64, FL), 1) % 64
        == lax.broadcasted_iota(jnp.int32, (64, FL), 0)
    ).astype(F32).astype(BF16)
    block = (
        lax.broadcasted_iota(jnp.int32, (CHD, FL), 0) // 16
        == lax.broadcasted_iota(jnp.int32, (CHD, FL), 1) // 64
    )
    signal = x_ref[...]
    for src, dst in ((inr_ref, ur), (ini_ref, ui)):
        total = None
        for piece in pieces(src[...]):
            wide = jnp.where(block, dot(piece, spread), 0.0).astype(BF16)
            term = dot(signal, wide)
            total = term if total is None else total + term
        dst[...] = total

    phase("barrier")
    pl.semaphore_wait(barrier, NT - 1 + NY - 1 + NZ - 1)

    phase("first_sends")
    gu.start_ya()
    gu.own_bz()
    gu.own_by()
    oproj.start(0)
    oproj.start(1)
    dn.own_bz()

    phase("scan")

    def tile_step(i, carry):
        for j in range(4):
            rows = pl.ds(pl.multiple_of(i * 32 + j * 8, 8), 8)
            v = cmul(ratio, (ur[rows, :], ui[rows, :]))
            for k, m in zip((1, 2, 4), masked):
                v = cadd(v, cmul(m, (pltpu.roll(v[0], k, 0), pltpu.roll(v[1], k, 0))))
            ur[rows, :] = v[0]
            ui[rows, :] = v[1]
            er[pl.ds(i * 4 + j, 1), :] = v[0][7:8]
            ei[pl.ds(i * 4 + j, 1), :] = v[1][7:8]
        return carry

    lax.fori_loop(0, TOK // 32, tile_step, 0)

    phase("ends")
    row64 = lax.broadcasted_iota(jnp.int32, (64, FL), 0)
    e = (er[...], ei[...])
    ladder = []
    p = powers[7]
    for k in (1, 2, 4, 8, 16, 32):
        ladder.append(p)
        moved = tuple(jnp.where(row64 >= k, pltpu.roll(v, k, 0), 0.0) for v in e)
        e = cadd(e, cmul(p, moved))
        p = cmul(p, p)
    er[...] = e[0]
    ei[...] = e[1]
    a512 = (packed(p[0]), packed(p[1]))
    last = (e[0][63:64], e[1][63:64])
    sb[y, 0:4, :] = packed(last[0])
    sb[y, 4:8, :] = packed(last[1])
    for k in range(1, NY):
        send(sb.at[y], sb.at[y], s_send.at[k], s_recv.at[y], sp_1=(y + k) % NY)
    dn.start_ya()

    phase("lead")
    lead = (jnp.ones((64, FL), F32), jnp.zeros((64, FL), F32))
    for b, q in enumerate(ladder):
        more = cmul(q, lead)
        bit = (row64 // (1 << b)) % 2 == 1
        lead = tuple(jnp.where(bit, m, v) for m, v in zip(more, lead))
    pcr[...] = lead[0]
    pci[...] = lead[1]

    phase("outmat")
    for k, (src, sign) in enumerate(((our_ref, 1.0), (oui_ref, -1.0))):
        hi, lo = pieces(src[...] * sign)
        mr[k] = jnp.where(block, dot(hi, spread), 0.0).astype(BF16)
        mi[k] = jnp.where(block, dot(lo, spread), 0.0).astype(BF16)

    phase("s_wait")
    for k in range(1, NY):
        yk = (y + k) % NY
        arrived(sb.at[yk], s_send.at[k], s_recv.at[yk], sp_1=yk)
    whole = (jnp.zeros((4, 128), F32), jnp.zeros((4, 128), F32))
    before = whole
    ahead = (jnp.ones((4, 128), F32), jnp.zeros((4, 128), F32))
    for b in range(NY):
        own_b = (sb[b, 0:4, :], sb[b, 4:8, :])
        whole = cadd(cmul(a512, whole), own_b)
        inside = b < y
        step_b = cadd(cmul(a512, before), own_b)
        before = tuple(jnp.where(inside, n, v) for n, v in zip(step_b, before))
        step_a = cmul(a512, ahead)
        ahead = tuple(jnp.where(inside, n, v) for n, v in zip(step_a, ahead))
    a2 = cmul(a512, a512)
    a4 = cmul(a2, a2)
    tb[z, 0:4, :] = whole[0]
    tb[z, 4:8, :] = whole[1]
    for k in range(1, NZ):
        send(tb.at[z], tb.at[z], t_send.at[k], t_recv.at[z], sp_0=(z + k) % NZ)

    phase("b1")
    gu.tick_b(1)
    phase("own_a")
    gu.own_a()
    phase("b2")
    gu.tick_y(0)
    gu.tick_b(2)
    phase("op0")
    oproj.forward(0)
    phase("y1")
    gu.tick_y(1)
    dn.tick_b(1)
    phase("a1")
    gu.tick_a(1, 0)
    gu.tick_a(1, 1)
    phase("b3")
    gu.tick_b(3)
    gu.tick_y(2)

    phase("t_wait")
    for k in range(1, NZ):
        zk = (z + k) % NZ
        arrived(tb.at[zk], t_send.at[k], t_recv.at[zk], sp_0=zk)
    phase("hold")
    hold = (jnp.zeros((4, 128), F32), jnp.zeros((4, 128), F32))
    for b in range(NZ - 1):
        step_h = cadd(cmul(a4, hold), (tb[b, 0:4, :], tb[b, 4:8, :]))
        hold = tuple(jnp.where(b < z, n, v) for n, v in zip(step_h, hold))
    hold = cadd(cmul(ahead, hold), before)
    hold = (flat(hold[0]), flat(hold[1]))
    enter = cmul((pcr[...], pci[...]), hold)
    prev = tuple(jnp.where(row64 >= 1, pltpu.roll(v[...], 1, 0), 0.0) for v in (er, ei))
    enter = cadd(enter, prev)
    pcr[...] = enter[0]
    pci[...] = enter[1]

    phase("read")

    def read_step(i, carry):
        re, im = [], []
        for j in range(16):
            k = i * 16 + j
            rows = pl.ds(pl.multiple_of(k * 8, 8), 8)
            w = (pcr[pl.ds(k, 1), :], pci[pl.ds(k, 1), :])
            v = cadd((ur[rows, :], ui[rows, :]), cmul(lift, w))
            re.append(v[0])
            im.append(v[1])
        total = None
        for k, v in enumerate((re, im)):
            hi, lo = pieces(jnp.concatenate(v, axis=0))
            term = dot_t(hi, mr[k]) + dot_t(hi, mi[k]) + dot_t(lo, mr[k])
            total = term if total is None else total + term
        rows = pl.ds(pl.multiple_of(i * 128, 128), 128)
        pre = total + skip_ref[...] * x_ref[rows, :].astype(F32)
        inner = 0.7978845608028654 * (pre + 0.044715 * (pre * pre * pre))
        val = (pre * (0.5 * (1.0 + jnp.tanh(inner)))).astype(BF16)
        act[2 * i] = val[0:64]
        act[2 * i + 1] = val[64:128]
        return carry

    lax.fori_loop(0, 4, read_step, 0)
    for k in range(1, NT):
        tk = (t + k) % NT
        send(act.at[tk], acts.at[t], a_send.at[k], a_recv.at[t], tp=tk)
    acts[t] = act[t]

    phase("op1")
    oproj.forward(1)
    phase("a2")
    gu.tick_a(2, 0)
    gu.tick_a(2, 1)
    phase("b4")
    gu.tick_b(4)
    gu.tick_y(3)
    oproj.last(0)
    phase("a3")
    gu.tick_a(3, 0)
    gu.tick_a(3, 1)
    dn.own_a()
    dn.own_by()
    phase("op_fin")
    oproj.last(1)
    oproj.finish(0)
    oproj.finish(1)

    phase("a_wait")
    for k in range(1, NT):
        tk = (t + k) % NT
        arrived(acts.at[tk], a_send.at[k], a_recv.at[tk], tp=tk)

    phase("mix")

    def mix_step(j, squares):
        cols = pl.ds(pl.multiple_of(j * 256, 256), 256)
        total = jnp.zeros((ROWS, 256), F32)
        for b in range(NT):
            total = total + dot(acts[b], opall[b, :, cols]).astype(BF16).astype(F32)
        v = res_ref[:, cols].astype(F32) + total.astype(BF16).astype(F32)
        carried[:, cols] = v
        return squares + jnp.sum(v * v, axis=1, keepdims=True)

    squares = lax.fori_loop(0, D // 512, mix_step, jnp.zeros((ROWS, 1), F32))
    gu.tick_b(5)
    gu.tick_y(4)
    squares = lax.fori_loop(D // 512, D // 256, mix_step, squares)
    scale = lax.rsqrt(squares * (1.0 / D) + 1e-06)
    nf[t] = (carried[...] * scale * gain_ref[...]).astype(BF16)
    norms.start(0)
    norms.start(1)
    phase("a4")
    gu.tick_a(4, 0)
    gu.tick_a(4, 1)
    dn.tick_b(2)
    phase("b6")
    gu.tick_b(6)
    gu.tick_y(5)
    phase("a5")
    gu.tick_a(5, 0)
    dn.tick_a(1, 0)
    gu.tick_a(5, 1)
    dn.tick_a(1, 1)
    phase("n0")
    norms.forward(0)
    phase("b7")
    gu.tick_b(7)
    gu.tick_y(6)
    dn.tick_b(3)
    dn.tick_y(0)
    phase("a6")
    gu.tick_a(6, 0)
    dn.tick_a(2, 0)
    gu.tick_a(6, 1)
    dn.tick_a(2, 1)
    phase("n1")
    norms.forward(1)
    norms.last(0)
    phase("b8")
    gu.tick_b(8)
    gu.tick_y(7)
    dn.tick_b(4)
    dn.tick_y(1)
    phase("a7")
    gu.tick_a(7, 0)
    dn.tick_a(3, 0)
    gu.tick_a(7, 1)
    dn.tick_a(3, 1)
    norms.last(1)
    gu.tick_y(8)
    dn.tick_y(2)
    phase("b5d")
    dn.tick_b(5)
    phase("a8")
    gu.tick_a(8, 0)
    dn.tick_a(4, 0)
    gu.tick_a(8, 1)
    dn.tick_a(4, 1)
    dn.tick_y(3)
    phase("n_fin")
    norms.finish(0)
    norms.finish(1)
    phase("g_fin")
    for s in range(0, HALF + 1):
        gu.finish(s)

    def up_step(j):
        w = jnp.concatenate(
            [wgu[:, :, j * 128 : (j + 1) * 128].reshape(D, 128),
             wgu[:, :, 640 + j * 128 : 768 + j * 128].reshape(D, 128)], axis=1
        )
        v = dot(nf[...].reshape(TOK, D), w)
        g = v[:, 0:128]
        hid[:, j * 128 : (j + 1) * 128] = (g / (1.0 + jnp.exp(-g)) * v[:, 128:256]).astype(BF16)

    phase("up0")
    up_step(0)
    up_step(1)
    phase("d5")
    dn.tick_b(6)
    dn.tick_y(4)
    dn.tick_a(5, 0)
    dn.tick_a(5, 1)
    dn.tick_y(5)
    phase("up1")
    up_step(2)
    up_step(3)
    phase("d6")
    dn.tick_b(7)
    dn.tick_a(6, 0)
    dn.tick_a(6, 1)
    dn.tick_y(6)
    phase("up2")
    up_step(4)
    v = dot(nf[...].reshape(TOK, D), wgu[:, :, 1280:1408].reshape(D, 128))
    v = v / (1.0 + jnp.exp(-v)) * pltpu.roll(v, 64, 1)
    low = lax.broadcasted_iota(jnp.int32, (TOK, 128), 1) < 64
    hid[:, 640:768] = jnp.where(low, v, 0.0).astype(BF16)

    def weights_of(zb):
        v = wdn[pl.ds(zb * NY, NY)]
        main = jnp.concatenate([v[:, :, 0:640], v[:, :, 640:1280]], axis=1).reshape(128, 640)
        tail = v[:, :, 1280:1408]
        turned = pltpu.roll(tail.reshape(64, 128).astype(F32), 64, 1).astype(BF16)
        tail = jnp.concatenate([tail, turned.reshape(NY, 16, 128)], axis=1).reshape(128, 128)
        return jnp.concatenate([main, tail], axis=1)

    def place(o):
        s = o // 2 + 1
        if s == HALF:
            return (z + HALF * (o % 2)) % NZ
        return (z + (s if o % 2 else NZ - s)) % NZ

    def down_step(i):
        w = jnp.concatenate([weights_of(place(2 * i)), weights_of(place(2 * i + 1))], axis=0)
        v = dot_t(hid[...], w)
        part[:, :, i * 256 : (i + 1) * 256] = v.astype(BF16).reshape(NT, ROWS, 256)

    xs = (net.x2, net.xm, net.xp, net.x)

    def span(k):
        return pl.ds(SPANS[k][0] * 256, (SPANS[k][1] - SPANS[k][0]) * 256)

    def sum_start(k):
        for i, xb in enumerate(xs):
            send(part.at[xb * 2 + net.other, :, span(k)], pr.at[xb, :, span(k)],
                 p_send.at[4 * k + i], p_recv.at[NX * k + xb], tp=net.tpo)

    def pair(k, xb):
        arrived(pr.at[xb, :, span(k)], p_send.at[0], p_recv.at[NX * k + xb], tp=net.tpo)
        mine = part[xb * 2 + net.c, :, span(k)].astype(F32)
        return mine + pr[xb, :, span(k)].astype(F32)

    def sum_pair(k):
        for i, (xb, to) in enumerate(((net.x2, net.tp2), (net.xm, net.tpm), (net.xp, net.tpp))):
            ps[i, :, span(k)] = pair(k, xb).astype(BF16)
            send(ps.at[i, :, span(k)], rs.at[i, :, span(k)],
                 r_send.at[3 * k + i], r_recv.at[3 * k + i], tp=to)

    def sum_finish(k):
        total = pair(k, net.x)
        for i, frm in enumerate((net.tp2, net.tpp, net.tpm)):
            arrived(rs.at[i, :, span(k)], r_send.at[0], r_recv.at[3 * k + i], tp=frm)
            total = total + rs[i, :, span(k)].astype(F32)
        total = total.astype(BF16).astype(F32)
        for i in range(2 * (SPANS[k][1] - SPANS[k][0])):
            cols = pl.ds(pl.multiple_of(place(2 * SPANS[k][0] + i) * 128, 128), 128)
            v = carried[:, cols] + 0.5 * total[:, i * 128 : (i + 1) * 128]
            out_ref[:, cols] = v.astype(BF16)

    phase("w0")
    dn.tick_b(8)
    dn.finish(1)
    down_step(0)
    dn.finish(2)
    down_step(1)
    phase("d7")
    dn.tick_a(7, 0)
    dn.tick_a(7, 1)
    dn.tick_y(7)
    dn.tick_y(8)
    phase("w2")
    dn.finish(3)
    down_step(2)
    sum_start(0)
    dn.finish(4)
    down_step(3)
    phase("w4")
    sum_pair(0)
    dn.finish(5)
    down_step(4)
    phase("w5")
    dn.finish(6)
    down_step(5)
    sum_start(1)
    phase("w6")
    dn.finish(7)
    down_step(6)
    sum_start(2)
    sum_pair(1)
    phase("d8")
    dn.tick_a(8, 0)
    dn.tick_a(8, 1)
    dn.finish(0)
    dn.finish(8)
    phase("w7")
    down_step(7)
    sum_start(3)
    phase("rs")
    sum_finish(0)
    sum_pair(2)
    sum_pair(3)
    sum_finish(1)
    sum_finish(2)
    sum_finish(3)

    phase("drain")
    for cp in net.sent:
        cp.wait_send()
    phase(None)


def on_device(
    mixer_in, residual, decay_real, decay_imag, log_step, in_real, in_imag,
    output_real, output_imaginary, skip, out_proj, norm_gain, w_gate, w_up, w_down,
):
    vmem = pltpu.VMEM
    dma = pltpu.SemaphoreType.DMA
    scratch = [
        vmem((NZ * NY, 32, GU), BF16),
        vmem((NZ * NY, 16, GU), BF16),
        vmem((NT, CHD, D), BF16),
        vmem((NY, 8, 128), F32),
        vmem((NZ, 8, 128), F32),
        vmem((NT, ROWS, CHD), BF16),
        vmem((NT, ROWS, CHD), BF16),
        vmem((NT, ROWS, D), BF16),
        vmem((TOK, 768), BF16),
        vmem((NT, ROWS, D), BF16),
        vmem((NX, ROWS, D), BF16),
        vmem((3, ROWS, D), BF16),
        vmem((3, ROWS, D), BF16),
        vmem((TOK, FL), F32),
        vmem((TOK, FL), F32),
        vmem((2, CHD, FL), BF16),
        vmem((2, CHD, FL), BF16),
        vmem((64, FL), F32),
        vmem((64, FL), F32),
        vmem((64, FL), F32),
        vmem((64, FL), F32),
        vmem((ROWS, D), F32),
    ]
    counts = RING_SEMS + RING_SEMS + [
        2 * NT, 14, 2 * NT, 14, NY, NY, NZ, NZ, NT, NT, NC * NX, NC * 4, NC * 3, NC * 3,
    ]
    scratch += [dma((n,)) for n in counts]
    return pl.pallas_call(
        kernel,
        out_shape=jax.ShapeDtypeStruct((ROWS, D), BF16),
        in_specs=[pl.BlockSpec(memory_space=vmem)] * 15,
        out_specs=pl.BlockSpec(memory_space=vmem),
        scratch_shapes=scratch,
        compiler_params=pltpu.CompilerParams(
            collective_id=0, has_side_effects=True, vmem_limit_bytes=60 * 1024 * 1024
        ),
    )(
        mixer_in, decay_real, decay_imag, log_step.reshape(1, 8),
        jnp.transpose(in_real, (0, 2, 1)).reshape(CHD, 64),
        jnp.transpose(in_imag, (0, 2, 1)).reshape(CHD, 64),
        output_real.reshape(CHD, 64), output_imaginary.reshape(CHD, 64),
        skip.reshape(1, CHD), out_proj, norm_gain.reshape(1, D),
        residual, w_gate, w_up, w_down.T,
    )


def solution(mesh):
    finer = Mesh(mesh.devices.reshape(NZ, NY, mesh.shape["tp"]), ("sp_0", "sp_1", "tp"))
    return jax.shard_map(
        on_device,
        mesh=finer,
        in_specs=(
            P(SP, "tp"),
            P(SP_TP, None),
            P("tp", None),
            P("tp", None),
            P("tp"),
            P("tp", None, None),
            P("tp", None, None),
            P("tp", None, None),
            P("tp", None, None),
            P("tp"),
            P("tp", None),
            P(),
            P(SP, "tp"),
            P(SP, "tp"),
            P("tp", SP),
        ),
        out_specs=P(SP_TP, None),
        check_vma=False,
    )
```

```python
import functools

import jax
import jax.numpy as jnp
from jax import lax
from jax.experimental import pallas as pl
from jax.experimental.pallas import tpu as pltpu
from jax.sharding import Mesh
from jax.sharding import PartitionSpec as P

SP = ("sp_0", "sp_1")
SP_TP = ("sp_0", "sp_1", "tp")
MESH = pl.DeviceIdType.MESH
F32 = jnp.float32
BF16 = jnp.bfloat16

NZ = 16
NY = 4
NX = 4
NT = 8
HALF = NZ // 2
EARLY = 12
D = 2048
TOK = 512
ROWS = TOK // NT
FL = 512
CHD = 128
FFD = 704
GU = 2 * FFD
CA = 512
SPANS = ((0, 2), (2, 4), (4, 6), (6, 8))
NC = len(SPANS)


def discrete(decay_real, decay_imag, log_step):
    step_size = jnp.exp(log_step)
    magnitude = jnp.exp(decay_real * step_size)
    angle = decay_imag * step_size
    power_re = magnitude * jnp.cos(angle)
    power_im = magnitude * jnp.sin(angle)
    denom = decay_real * decay_real + decay_imag * decay_imag
    ratio_re = ((power_re - 1.0) * decay_real + power_im * decay_imag) / denom
    ratio_im = (power_im * decay_real - (power_re - 1.0) * decay_imag) / denom
    return (power_re, power_im), (ratio_re, ratio_im)


def cmul(a, b):
    return (a[0] * b[0] - a[1] * b[1], a[0] * b[1] + a[1] * b[0])


def cadd(a, b):
    return (a[0] + b[0], a[1] + b[1])


def pieces(v):
    hi = v.astype(BF16)
    lo = (v - hi.astype(F32)).astype(BF16)
    return hi, lo


def dot(a, b):
    return jnp.dot(a, b, preferred_element_type=F32)


def dot_t(a, b):
    return lax.dot_general(a, b, (((1,), (1,)), ((), ())), preferred_element_type=F32)


def packed(row):
    return jnp.concatenate([row[:, i * 128 : (i + 1) * 128] for i in range(4)], axis=0)


def flat(block):
    return jnp.concatenate([block[i : i + 1] for i in range(4)], axis=1)


class Phase:
    def __init__(self):
        self.scope = None

    def __call__(self, name):
        if self.scope is not None:
            self.scope.__exit__(None, None, None)
        self.scope = None
        if name:
            self.scope = jax.named_scope(name)
            self.scope.__enter__()


class Ring:
    count = 33

    def __init__(self, net, buf, sems):
        self.net, self.buf = net, buf
        (self.ya_recv, self.ya_send, self.za_recv, self.za_send,
         self.zb_recv, self.zb_send, self.yb_recv, self.yb_send) = sems

    def a_y(self, zb, yb):
        return self.buf.at[zb * NY + yb, :, 0:CA]

    def a_z(self, zb, h):
        return self.buf.at[pl.ds(zb * NY + 2 * h, 2), :, 0:CA]

    def b(self, zb, yb):
        return self.buf.at[zb * NY + yb, :, CA:GU]

    def start_ya(self):
        n = self.net
        blk = self.a_y(n.z, n.y)
        for k in range(1, NY):
            n.send(blk, blk, self.ya_send.at[k], self.ya_recv.at[n.y], sp_1=(n.y + k) % NY)

    def finish_ya(self):
        n = self.net
        for k in range(1, NY):
            yk = (n.y + k) % NY
            n.arrived(self.a_y(n.z, yk), self.ya_send.at[k], self.ya_recv.at[yk], sp_1=yk)

    def forward_a(self, zb, chain, s, h):
        n = self.net
        blk = self.a_z(zb, h)
        n.send(blk, blk, self.za_send.at[(chain * HALF + s) * 2 + h], self.za_recv.at[zb * 2 + h],
               sp_0=n.zp if chain == 0 else n.zm)

    def forward_b(self, zb, chain, s):
        n = self.net
        blk = self.b(zb, n.y)
        n.send(blk, blk, self.zb_send.at[chain * HALF + s], self.zb_recv.at[zb],
               sp_0=n.zp if chain == 0 else n.zm)

    def start_yb(self, zb, o):
        n = self.net
        blk = self.b(zb, n.y)
        sem = self.yb_recv.at[zb * NY + n.y]
        n.send(blk, blk, self.yb_send.at[3 * o], sem, sp_1=n.yp)
        n.send(blk, blk, self.yb_send.at[3 * o + 1], sem, sp_1=n.ym)

    def own_a(self):
        self.finish_ya()
        for h in (0, 1):
            for chain in (0, 1):
                self.forward_a(self.net.z, chain, 0, h)

    def own_bz(self):
        for chain in (0, 1):
            self.forward_b(self.net.z, chain, 0)

    def own_by(self):
        self.start_yb(self.net.z, 0)

    def tick_a(self, s, h):
        n = self.net
        for chain in n.chains(s):
            zb = n.block(chain, s)
            n.arrived(self.a_z(zb, h), self.za_send.at[0], self.za_recv.at[zb * 2 + h], sp_0=n.zm)
            if n.goes_on(chain, s):
                self.forward_a(zb, chain, s, h)

    def tick_b(self, s):
        n = self.net
        for chain in n.chains(s):
            zb = n.block(chain, s)
            n.arrived(self.b(zb, n.y), self.zb_send.at[0], self.zb_recv.at[zb], sp_0=n.zm)
            if n.goes_on(chain, s):
                self.forward_b(zb, chain, s)
            self.start_yb(zb, n.order(chain, s))

    def tick_y(self, s):
        n = self.net
        for chain in n.chains(s):
            zb, o = n.block(chain, s), n.order(chain, s)
            blk = self.b(zb, n.ym)
            sem = self.yb_recv.at[zb * NY + n.ym]
            n.arrived(blk, self.yb_send.at[3 * o + 2], sem, sp_1=n.ym)
            n.send(blk, blk, self.yb_send.at[3 * o + 2], sem, sp_1=n.yp)

    def finish(self, s):
        n = self.net
        for chain in n.chains(s):
            zb, o = n.block(chain, s), n.order(chain, s)
            for yb in (n.yp, n.y2):
                n.arrived(self.b(zb, yb), self.yb_send.at[3 * o],
                          self.yb_recv.at[zb * NY + yb], sp_1=n.yp)


RING_SEMS = [NY, NY, 2 * NZ, 4 * HALF, NZ, NZ, NZ * NY, 3 * NZ]


class Pool:
    def __init__(self, net, buf, recv, ssem):
        self.net, self.buf, self.recv, self.ssem = net, buf, recv, ssem

    def at(self, b, h):
        return self.buf.at[b, :, h * (D // 2) : (h + 1) * (D // 2)]

    def put(self, b, h, k, to):
        blk = self.at(b, h)
        self.net.send(blk, blk, self.ssem.at[2 * k + h], self.recv.at[b * 2 + h], tp=to)

    def get(self, b, h, frm):
        self.net.arrived(self.at(b, h), self.ssem.at[0], self.recv.at[b * 2 + h], tp=frm)

    def start(self, h):
        n = self.net
        self.put(n.t, h, 0, n.tpp)
        self.put(n.t, h, 1, n.tpm)
        self.put(n.t, h, 2, n.tpo)

    def forward(self, h):
        n = self.net
        self.get(n.tpm, h, n.tpm)
        self.put(n.tpm, h, 3, n.tpp)
        self.put(n.tpm, h, 4, n.tpo)
        self.get(n.tpp, h, n.tpp)
        self.put(n.tpp, h, 5, n.tpo)

    def last(self, h):
        n = self.net
        self.get(n.tp2, h, n.tpm)
        self.put(n.tp2, h, 6, n.tpo)

    def finish(self, h):
        n = self.net
        for xb in (n.x, n.xp, n.xm, n.x2):
            self.get(xb * 2 + n.other, h, n.tpo)


class Net:
    def __init__(self):
        self.z = lax.axis_index("sp_0")
        self.y = lax.axis_index("sp_1")
        self.t = lax.axis_index("tp")
        z, y, t = self.z, self.y, self.t
        x, c = t // 2, t % 2
        self.x, self.c = x, c
        self.yp = (y + 1 + 2 * c) % NY
        self.ym = (y + 3 + 2 * c) % NY
        self.y2 = (y + 2) % NY
        self.zp = (z + 1 + (NZ - 2) * c) % NZ
        self.zm = (z + NZ - 1 + 2 * c) % NZ
        self.xp = (x + 1 + 2 * c) % NX
        self.xm = (x + 3 + 2 * c) % NX
        self.x2 = (x + 2) % NX
        self.other = 1 - c
        self.tpp = self.xp * 2 + c
        self.tpm = self.xm * 2 + c
        self.tp2 = self.x2 * 2 + c
        self.tpo = x * 2 + self.other
        self.sent = []

    def copy(self, src, dst, ss, rs, **dev):
        return pltpu.make_async_remote_copy(
            src_ref=src, dst_ref=dst, send_sem=ss, recv_sem=rs, device_id=dev, device_id_type=MESH
        )

    def send(self, src, dst, ss, rs, **dev):
        cp = self.copy(src, dst, ss, rs, **dev)
        cp.start()
        self.sent.append(cp)

    def arrived(self, dst, ss, rs, **dev):
        self.copy(dst, dst, ss, rs, **dev).wait_recv()

    def chains(self, s):
        return (0,) if s in (0, HALF) else (0, 1)

    def goes_on(self, chain, s):
        return s < (HALF if chain == 0 else HALF - 1)

    def block(self, chain, s):
        toward = self.zm - self.z if chain == 0 else self.zp - self.z
        return (self.z + NZ * NZ + s * toward) % NZ

    def order(self, chain, s):
        return 0 if s == 0 else 2 * s - 1 + chain


def kernel(
    x_ref, dr_ref, di_ref, ls_ref, inr_ref, ini_ref, our_ref, oui_ref, skip_ref, op_ref, gain_ref,
    res_ref, wg_ref, wu_ref, wd_ref, out_ref,
    wgu, wdn, opall, sb, tb, act, acts, nf, hid, part, pr, ps, rs,
    ur, ui, mr, mi, er, ei, pcr, pci, carried, acc, *sems,
):
    net = Net()
    phase = Phase()
    z, y, t = net.z, net.y, net.t
    send, arrived = net.send, net.arrived
    gu = Ring(net, wgu, sems[0:8])
    dn = Ring(net, wdn, sems[8:16])
    (o_recv, o_send, n_recv, n_send, s_recv, s_send, t_recv, t_send, a_recv, a_send,
     p_recv, p_send, r_recv, r_send) = sems[16:]
    oproj = Pool(net, opall, o_recv, o_send)
    norms = Pool(net, nf, n_recv, n_send)

    phase("signal")
    barrier = pltpu.get_barrier_semaphore()
    for k in range(1, NZ):
        pl.semaphore_signal(barrier, inc=1, device_id={"sp_0": (z + k) % NZ}, device_id_type=MESH)
    for k in range(1, NY):
        pl.semaphore_signal(barrier, inc=1, device_id={"sp_1": (y + k) % NY}, device_id_type=MESH)
    for k in range(1, NT):
        pl.semaphore_signal(barrier, inc=1, device_id={"tp": (t + k) % NT}, device_id_type=MESH)

    phase("own")
    own = z * NY + y
    wgu[own, :, 0:640] = wg_ref[:, 0:640]
    wgu[own, :, 640:1280] = wu_ref[:, 0:640]
    wgu[own, :, 1280:1408] = jnp.concatenate([wg_ref[:, 640:704], wu_ref[:, 640:704]], axis=1)
    wdn[own, :, 0:640] = wd_ref[0:16, 0:640]
    wdn[own, :, 640:1280] = wd_ref[16:32, 0:640]
    wdn[own, :, 1280:1408] = jnp.concatenate([wd_ref[0:16, 640:704], wd_ref[16:32, 640:704]], axis=1)
    opall[t] = op_ref[...]

    phase("coef")
    eight = lax.broadcasted_iota(jnp.int32, (8, 8), 0) == lax.broadcasted_iota(jnp.int32, (8, 8), 1)
    log_step = jnp.sum(
        jnp.where(eight, jnp.broadcast_to(ls_ref[...], (8, 8)), 0.0), axis=1, keepdims=True
    )
    a, ratio = discrete(dr_ref[...], di_ref[...], log_step)

    def line(v):
        return jnp.concatenate([v[g : g + 1] for g in range(8)], axis=1)

    a = (line(a[0]), line(a[1]))
    ratio = (line(ratio[0]), line(ratio[1]))
    powers = [a]
    for _ in range(7):
        powers.append(cmul(powers[-1], a))
    lift = tuple(jnp.concatenate([p[i] for p in powers], axis=0) for i in (0, 1))
    row8 = lax.broadcasted_iota(jnp.int32, (8, FL), 0)
    masked = []
    for k in (1, 2, 4):
        p = powers[k - 1]
        masked.append(tuple(jnp.where(row8 >= k, jnp.broadcast_to(v, (8, FL)), 0.0) for v in p))

    phase("drive")
    spread = (
        lax.broadcasted_iota(jnp.int32, (64, FL), 1) % 64
        == lax.broadcasted_iota(jnp.int32, (64, FL), 0)
    ).astype(F32).astype(BF16)
    block = (
        lax.broadcasted_iota(jnp.int32, (CHD, FL), 0) // 16
        == lax.broadcasted_iota(jnp.int32, (CHD, FL), 1) // 64
    )
    signal = x_ref[...]
    for src, dst in ((inr_ref, ur), (ini_ref, ui)):
        total = None
        for piece in pieces(src[...]):
            wide = jnp.where(block, dot(piece, spread), 0.0).astype(BF16)
            term = dot(signal, wide)
            total = term if total is None else total + term
        dst[...] = total

    phase("scan")

    def tile_step(i, carry):
        for j in range(4):
            rows = pl.ds(pl.multiple_of(i * 32 + j * 8, 8), 8)
            v = cmul(ratio, (ur[rows, :], ui[rows, :]))
            for k, m in zip((1, 2, 4), masked):
                v = cadd(v, cmul(m, (pltpu.roll(v[0], k, 0), pltpu.roll(v[1], k, 0))))
            ur[rows, :] = v[0]
            ui[rows, :] = v[1]
            er[pl.ds(i * 4 + j, 1), :] = v[0][7:8]
            ei[pl.ds(i * 4 + j, 1), :] = v[1][7:8]
        return carry

    lax.fori_loop(0, TOK // 32, tile_step, 0)

    phase("ends")
    row64 = lax.broadcasted_iota(jnp.int32, (64, FL), 0)
    e = (er[...], ei[...])
    ladder = []
    p = powers[7]
    for k in (1, 2, 4, 8, 16, 32):
        ladder.append(p)
        moved = tuple(jnp.where(row64 >= k, pltpu.roll(v, k, 0), 0.0) for v in e)
        e = cadd(e, cmul(p, moved))
        p = cmul(p, p)
    er[...] = e[0]
    ei[...] = e[1]
    a512 = (packed(p[0]), packed(p[1]))
    last = (e[0][63:64], e[1][63:64])
    sb[y, 0:4, :] = packed(last[0])
    sb[y, 4:8, :] = packed(last[1])
    phase("lead")
    lead = (jnp.ones((64, FL), F32), jnp.zeros((64, FL), F32))
    for b, q in enumerate(ladder):
        more = cmul(q, lead)
        bit = (row64 // (1 << b)) % 2 == 1
        lead = tuple(jnp.where(bit, m, v) for m, v in zip(more, lead))
    pcr[...] = lead[0]
    pci[...] = lead[1]

    phase("outmat")
    for k, (src, sign) in enumerate(((our_ref, 1.0), (oui_ref, -1.0))):
        hi, lo = pieces(src[...] * sign)
        mr[k] = jnp.where(block, dot(hi, spread), 0.0).astype(BF16)
        mi[k] = jnp.where(block, dot(lo, spread), 0.0).astype(BF16)

    phase("barrier")
    pl.semaphore_wait(barrier, NT - 1 + NY - 1 + NZ - 1)

    phase("first_sends")
    for k in range(1, NY):
        send(sb.at[y], sb.at[y], s_send.at[k], s_recv.at[y], sp_1=(y + k) % NY)
    gu.own_bz()
    gu.start_ya()
    oproj.start(0)
    oproj.start(1)
    gu.own_by()

    phase("b1")
    gu.tick_b(1)
    phase("s_wait")
    for k in range(1, NY):
        yk = (y + k) % NY
        arrived(sb.at[yk], s_send.at[k], s_recv.at[yk], sp_1=yk)
    whole = (jnp.zeros((4, 128), F32), jnp.zeros((4, 128), F32))
    before = whole
    ahead = (jnp.ones((4, 128), F32), jnp.zeros((4, 128), F32))
    for b in range(NY):
        own_b = (sb[b, 0:4, :], sb[b, 4:8, :])
        whole = cadd(cmul(a512, whole), own_b)
        inside = b < y
        step_b = cadd(cmul(a512, before), own_b)
        before = tuple(jnp.where(inside, n, v) for n, v in zip(step_b, before))
        step_a = cmul(a512, ahead)
        ahead = tuple(jnp.where(inside, n, v) for n, v in zip(step_a, ahead))
    a2 = cmul(a512, a512)
    a4 = cmul(a2, a2)
    tb[z, 0:4, :] = whole[0]
    tb[z, 4:8, :] = whole[1]
    for k in range(1, NZ):
        cp = net.copy(tb.at[z], tb.at[z], t_send.at[k], t_recv.at[z], sp_0=(z + k) % NZ)

        @pl.when(z + k < NZ)
        def _():
            cp.start()


    phase("own_a")
    gu.own_a()
    phase("b2")
    gu.tick_b(2)
    gu.tick_y(0)
    phase("a1")
    gu.tick_a(1, 0)
    phase("op0")
    oproj.forward(0)
    phase("a1b")
    gu.tick_a(1, 1)
    phase("b3")
    gu.tick_b(3)
    gu.tick_y(1)

    phase("op1")
    oproj.forward(1)

    phase("t_wait")
    for b in range(NZ - 1):

        @pl.when(b < z)
        def _():
            arrived(tb.at[b], t_send.at[1], t_recv.at[b], sp_0=b)

    phase("hold")
    hold = (jnp.zeros((4, 128), F32), jnp.zeros((4, 128), F32))
    for b in range(NZ - 1):
        step_h = cadd(cmul(a4, hold), (tb[b, 0:4, :], tb[b, 4:8, :]))
        hold = tuple(jnp.where(b < z, n, v) for n, v in zip(step_h, hold))
    hold = cadd(cmul(ahead, hold), before)
    hold = (flat(hold[0]), flat(hold[1]))
    enter = cmul((pcr[...], pci[...]), hold)
    prev = tuple(jnp.where(row64 >= 1, pltpu.roll(v[...], 1, 0), 0.0) for v in (er, ei))
    enter = cadd(enter, prev)
    pcr[...] = enter[0]
    pci[...] = enter[1]

    phase("read")

    def read_step(i, carry):
        re, im = [], []
        for j in range(16):
            k = i * 16 + j
            rows = pl.ds(pl.multiple_of(k * 8, 8), 8)
            w = (pcr[pl.ds(k, 1), :], pci[pl.ds(k, 1), :])
            v = cadd((ur[rows, :], ui[rows, :]), cmul(lift, w))
            re.append(v[0])
            im.append(v[1])
        total = None
        for k, v in enumerate((re, im)):
            hi, lo = pieces(jnp.concatenate(v, axis=0))
            term = dot_t(hi, mr[k]) + dot_t(hi, mi[k]) + dot_t(lo, mr[k])
            total = term if total is None else total + term
        rows = pl.ds(pl.multiple_of(i * 128, 128), 128)
        pre = total + skip_ref[...] * x_ref[rows, :].astype(F32)
        inner = 0.7978845608028654 * (pre + 0.044715 * (pre * pre * pre))
        val = (pre * (0.5 * (1.0 + jnp.tanh(inner)))).astype(BF16)
        act[2 * i] = val[0:64]
        act[2 * i + 1] = val[64:128]
        return carry

    lax.fori_loop(0, 4, read_step, 0)
    for k in range(1, NT):
        tk = (t + k) % NT
        send(act.at[tk], acts.at[t], a_send.at[k], a_recv.at[t], tp=tk)
    acts[t] = act[t]

    phase("a2")
    gu.tick_a(2, 0)
    gu.tick_a(2, 1)
    phase("b4")
    gu.tick_b(4)
    phase("y2")
    gu.tick_y(2)
    dn.start_ya()
    phase("a3")
    gu.tick_a(3, 0)
    dn.own_bz()
    gu.tick_a(3, 1)
    phase("op_last")
    oproj.last(0)
    oproj.last(1)
    phase("b5")
    gu.tick_b(5)
    gu.tick_y(3)
    phase("op_fin")
    oproj.finish(0)
    oproj.finish(1)

    phase("a_wait")
    for k in range(1, NT):
        tk = (t + k) % NT
        arrived(acts.at[tk], a_send.at[k], a_recv.at[tk], tp=tk)

    def near(o):
        s = (o + 1) // 2
        return (z + (NZ - s if o % 2 else s)) % NZ

    def up_dot(lo, hi, *cols):
        parts = []
        for c in cols:
            blocks = [wgu[pl.ds(near(o) * NY, NY), :, c : c + 128].reshape(128, 128) for o in range(lo, hi)]
            parts.append(jnp.concatenate(blocks, axis=0))
        w = parts[0] if len(parts) == 1 else jnp.concatenate(parts, axis=1)
        return dot(nf[:, :, lo * 128 : hi * 128].reshape(TOK, (hi - lo) * 128), w)

    def up_early(j):
        acc[:, j * 256 : (j + 1) * 256] = up_dot(0, EARLY, j * 128, 640 + j * 128)

    def up_step(j):
        v = acc[:, j * 256 : (j + 1) * 256] + up_dot(EARLY, NZ, j * 128, 640 + j * 128)
        g = v[:, 0:128]
        hid[:, j * 128 : (j + 1) * 128] = (g / (1.0 + jnp.exp(-g)) * v[:, 128:256]).astype(BF16)

    phase("mix")

    def mix_step(j, squares):
        cols = pl.ds(pl.multiple_of(j * 256, 256), 256)
        total = jnp.zeros((ROWS, 256), F32)
        for b in range(NT):
            total = total + dot(acts[b], opall[b, :, cols]).astype(BF16).astype(F32)
        v = res_ref[:, cols].astype(F32) + total.astype(BF16).astype(F32)
        carried[:, cols] = v
        return squares + jnp.sum(v * v, axis=1, keepdims=True)

    squares = lax.fori_loop(0, D // 512, mix_step, jnp.zeros((ROWS, 1), F32))
    gu.tick_a(4, 0)
    gu.tick_a(4, 1)
    dn.own_a()
    squares = lax.fori_loop(D // 512, D // 256, mix_step, squares)
    scale = lax.rsqrt(squares * (1.0 / D) + 1e-06)
    for o in range(NZ):
        src = pl.ds(pl.multiple_of(near(o) * 128, 128), 128)
        nf[t, :, o * 128 : (o + 1) * 128] = (carried[:, src] * scale * gain_ref[:, src]).astype(BF16)
    norms.start(0)
    norms.start(1)
    phase("b6")
    gu.tick_b(6)
    gu.tick_y(4)
    dn.tick_b(1)
    dn.own_by()
    phase("a5")
    gu.tick_a(5, 0)
    gu.tick_a(5, 1)
    dn.tick_a(1, 0)
    phase("n0")
    norms.forward(0)
    phase("b7")
    dn.tick_a(1, 1)
    gu.tick_b(7)
    gu.tick_y(5)
    dn.tick_b(2)
    phase("n1")
    norms.forward(1)
    phase("a6")
    gu.tick_a(6, 0)
    dn.tick_a(2, 0)
    gu.tick_a(6, 1)
    dn.tick_a(2, 1)
    norms.last(0)
    phase("b8")
    gu.tick_b(8)
    gu.tick_y(6)
    dn.tick_b(3)
    dn.tick_y(0)
    norms.last(1)
    phase("a7")
    gu.tick_a(7, 0)
    dn.tick_a(3, 0)
    gu.tick_a(7, 1)
    dn.tick_a(3, 1)
    gu.tick_y(7)
    dn.tick_b(4)
    dn.tick_y(1)
    phase("n_fin")
    norms.finish(0)
    norms.finish(1)
    for s in range(0, 7):
        gu.finish(s)
    phase("early0")
    up_early(0)
    up_early(1)
    phase("a8")
    gu.tick_a(8, 0)
    gu.tick_y(8)
    gu.tick_a(8, 1)
    dn.tick_a(4, 0)
    dn.tick_a(4, 1)
    dn.tick_b(5)
    dn.tick_y(2)
    phase("early1")
    up_early(2)
    up_early(3)
    phase("d5")
    dn.tick_a(5, 0)
    dn.tick_a(5, 1)
    dn.tick_b(6)
    dn.tick_y(3)
    phase("early2")
    up_early(4)
    acc[:, 1280:1408] = up_dot(0, EARLY, 1280)
    phase("g_fin")
    for s in range(7, HALF + 1):
        gu.finish(s)

    phase("up0")
    for j in range(4):
        up_step(j)
    phase("d6")
    dn.tick_a(6, 0)
    dn.tick_a(6, 1)
    dn.tick_b(7)
    dn.tick_y(4)
    phase("up2")
    up_step(4)
    v = acc[:, 1280:1408] + up_dot(EARLY, NZ, 1280)
    v = v / (1.0 + jnp.exp(-v)) * pltpu.roll(v, 64, 1)
    low = lax.broadcasted_iota(jnp.int32, (TOK, 128), 1) < 64
    hid[:, 640:768] = jnp.where(low, v, 0.0).astype(BF16)

    def weights_of(zb):
        v = wdn[pl.ds(zb * NY, NY)]
        main = jnp.concatenate([v[:, :, 0:640], v[:, :, 640:1280]], axis=1).reshape(128, 640)
        tail = v[:, :, 1280:1408]
        turned = pltpu.roll(tail.reshape(64, 128).astype(F32), 64, 1).astype(BF16)
        tail = jnp.concatenate([tail, turned.reshape(NY, 16, 128)], axis=1).reshape(128, 128)
        return jnp.concatenate([main, tail], axis=1)

    def place(o):
        s = o // 2 + 1
        if s == HALF:
            return (z + HALF * (o % 2)) % NZ
        return (z + (s if o % 2 else NZ - s)) % NZ

    def down_step(i):
        w = jnp.concatenate([weights_of(place(2 * i)), weights_of(place(2 * i + 1))], axis=0)
        v = dot_t(hid[...], w)
        part[:, :, i * 256 : (i + 1) * 256] = v.astype(BF16).reshape(NT, ROWS, 256)

    xs = (net.x2, net.xm, net.xp, net.x)

    def span(k):
        return pl.ds(SPANS[k][0] * 256, (SPANS[k][1] - SPANS[k][0]) * 256)

    def sum_start(k):
        for i, xb in enumerate(xs):
            send(part.at[xb * 2 + net.other, :, span(k)], pr.at[xb, :, span(k)],
                 p_send.at[4 * k + i], p_recv.at[NX * k + xb], tp=net.tpo)

    def pair(k, xb):
        arrived(pr.at[xb, :, span(k)], p_send.at[0], p_recv.at[NX * k + xb], tp=net.tpo)
        mine = part[xb * 2 + net.c, :, span(k)].astype(F32)
        return mine + pr[xb, :, span(k)].astype(F32)

    def hop(k, i, value, to):
        ps[i, :, span(k)] = value.astype(BF16)
        send(ps.at[i, :, span(k)], rs.at[i, :, span(k)],
             r_send.at[3 * k + i], r_recv.at[3 * k + i], tp=to)

    def landed(k, i, frm):
        arrived(rs.at[i, :, span(k)], r_send.at[0], r_recv.at[3 * k + i], tp=frm)
        return rs[i, :, span(k)].astype(F32)

    def sum_pair(k):
        hop(k, 0, pair(k, net.x2), net.tp2 if k == NC - 1 else net.tpp)
        hop(k, 1, pair(k, net.xm), net.tpm)
        if k == NC - 1:
            hop(k, 2, pair(k, net.xp), net.tpp)

    def sum_relay(k):
        near = pair(k, net.xp)
        hop(k, 2, near + landed(k, 0, net.tpm), net.tpp)

    def sum_finish(k):
        total = pair(k, net.x) + landed(k, 1, net.tpp) + landed(k, 2, net.tpm)
        if k == NC - 1:
            total = total + landed(k, 0, net.tp2)
        total = total.astype(BF16).astype(F32)
        for i in range(2 * (SPANS[k][1] - SPANS[k][0])):
            cols = pl.ds(pl.multiple_of(place(2 * SPANS[k][0] + i) * 128, 128), 128)
            v = carried[:, cols] + 0.5 * total[:, i * 128 : (i + 1) * 128]
            out_ref[:, cols] = v.astype(BF16)

    phase("w0")
    dn.finish(1)
    down_step(0)
    dn.finish(2)
    down_step(1)
    sum_start(0)
    phase("w2")
    dn.finish(3)
    down_step(2)
    sum_pair(0)
    phase("d7")
    dn.tick_y(5)
    dn.tick_a(7, 0)
    dn.tick_a(7, 1)
    dn.tick_b(8)
    dn.tick_y(6)
    phase("w3")
    dn.finish(4)
    down_step(3)
    sum_start(1)
    phase("d8")
    dn.tick_y(7)
    dn.tick_a(8, 0)
    dn.tick_a(8, 1)
    dn.tick_y(8)
    phase("w4")
    sum_relay(0)
    sum_pair(1)
    phase("w4d")
    dn.finish(5)
    down_step(4)
    dn.finish(6)
    down_step(5)
    sum_start(2)
    phase("w6")
    dn.finish(7)
    down_step(6)
    phase("w7")
    dn.finish(0)
    dn.finish(8)
    down_step(7)
    sum_start(3)
    phase("pair2")
    sum_pair(2)
    sum_relay(1)
    phase("pair3")
    sum_pair(3)
    sum_finish(0)
    phase("relay2")
    sum_relay(2)
    sum_finish(1)
    phase("rs2")
    sum_finish(2)
    phase("rs3")
    sum_finish(3)

    phase("drain")
    for cp in net.sent:
        cp.wait_send()
    for k in range(1, NZ):

        @pl.when(z + k < NZ)
        def _():
            net.copy(tb.at[z], tb.at[z], t_send.at[k], t_recv.at[z], sp_0=(z + k) % NZ).wait_send()

    phase(None)


def on_device(
    mixer_in, residual, decay_real, decay_imag, log_step, in_real, in_imag,
    output_real, output_imaginary, skip, out_proj, norm_gain, w_gate, w_up, w_down,
):
    vmem = pltpu.VMEM
    dma = pltpu.SemaphoreType.DMA
    scratch = [
        vmem((NZ * NY, 32, GU), BF16),
        vmem((NZ * NY, 16, GU), BF16),
        vmem((NT, CHD, D), BF16),
        vmem((NY, 8, 128), F32),
        vmem((NZ, 8, 128), F32),
        vmem((NT, ROWS, CHD), BF16),
        vmem((NT, ROWS, CHD), BF16),
        vmem((NT, ROWS, D), BF16),
        vmem((TOK, 768), BF16),
        vmem((NT, ROWS, D), BF16),
        vmem((NX, ROWS, D), BF16),
        vmem((3, ROWS, D), BF16),
        vmem((3, ROWS, D), BF16),
        vmem((TOK, FL), F32),
        vmem((TOK, FL), F32),
        vmem((2, CHD, FL), BF16),
        vmem((2, CHD, FL), BF16),
        vmem((64, FL), F32),
        vmem((64, FL), F32),
        vmem((64, FL), F32),
        vmem((64, FL), F32),
        vmem((ROWS, D), F32),
        vmem((TOK, GU), F32),
    ]
    counts = RING_SEMS + RING_SEMS + [
        2 * NT, 14, 2 * NT, 14, NY, NY, NZ, NZ, NT, NT, NC * NX, NC * 4, NC * 3, NC * 3,
    ]
    scratch += [dma((n,)) for n in counts]
    return pl.pallas_call(
        kernel,
        out_shape=jax.ShapeDtypeStruct((ROWS, D), BF16),
        in_specs=[pl.BlockSpec(memory_space=vmem)] * 15,
        out_specs=pl.BlockSpec(memory_space=vmem),
        scratch_shapes=scratch,
        compiler_params=pltpu.CompilerParams(
            collective_id=0, has_side_effects=True, vmem_limit_bytes=60 * 1024 * 1024
        ),
    )(
        mixer_in, decay_real, decay_imag, log_step.reshape(1, 8),
        jnp.transpose(in_real, (0, 2, 1)).reshape(CHD, 64),
        jnp.transpose(in_imag, (0, 2, 1)).reshape(CHD, 64),
        output_real.reshape(CHD, 64), output_imaginary.reshape(CHD, 64),
        skip.reshape(1, CHD), out_proj, norm_gain.reshape(1, D),
        residual, w_gate, w_up, w_down.T,
    )


def solution(mesh):
    finer = Mesh(mesh.devices.reshape(NZ, NY, mesh.shape["tp"]), ("sp_0", "sp_1", "tp"))
    return jax.shard_map(
        on_device,
        mesh=finer,
        in_specs=(
            P(SP, "tp"),
            P(SP_TP, None),
            P("tp", None),
            P("tp", None),
            P("tp"),
            P("tp", None, None),
            P("tp", None, None),
            P("tp", None, None),
            P("tp", None, None),
            P("tp"),
            P("tp", None),
            P(),
            P(SP, "tp"),
            P(SP, "tp"),
            P("tp", SP),
        ),
        out_specs=P(SP_TP, None),
        check_vma=False,
    )
```

```python
import functools

import jax
import jax.numpy as jnp
from jax import lax
from jax.experimental import pallas as pl
from jax.experimental.pallas import tpu as pltpu
from jax.sharding import Mesh
from jax.sharding import PartitionSpec as P

SP = ("sp_0", "sp_1")
SP_TP = ("sp_0", "sp_1", "tp")
MESH = pl.DeviceIdType.MESH
F32 = jnp.float32
BF16 = jnp.bfloat16

NZ = 16
NY = 4
NX = 4
NT = 8
HALF = NZ // 2
EARLY = 12
D = 2048
TOK = 512
ROWS = TOK // NT
FL = 512
CHD = 128
FFD = 704
GU = 2 * FFD
CA = 512
SPANS = ((0, 2), (2, 4), (4, 6), (6, 8))
NC = len(SPANS)
STRAIGHT = 1


def discrete(decay_real, decay_imag, log_step):
    step_size = jnp.exp(log_step)
    magnitude = jnp.exp(decay_real * step_size)
    angle = decay_imag * step_size
    power_re = magnitude * jnp.cos(angle)
    power_im = magnitude * jnp.sin(angle)
    denom = decay_real * decay_real + decay_imag * decay_imag
    ratio_re = ((power_re - 1.0) * decay_real + power_im * decay_imag) / denom
    ratio_im = (power_im * decay_real - (power_re - 1.0) * decay_imag) / denom
    return (power_re, power_im), (ratio_re, ratio_im)


def cmul(a, b):
    return (a[0] * b[0] - a[1] * b[1], a[0] * b[1] + a[1] * b[0])


def cadd(a, b):
    return (a[0] + b[0], a[1] + b[1])


def pieces(v):
    hi = v.astype(BF16)
    lo = (v - hi.astype(F32)).astype(BF16)
    return hi, lo


def dot(a, b):
    return jnp.dot(a, b, preferred_element_type=F32)


def dot_t(a, b):
    return lax.dot_general(a, b, (((1,), (1,)), ((), ())), preferred_element_type=F32)


def packed(row):
    return jnp.concatenate([row[:, i * 128 : (i + 1) * 128] for i in range(4)], axis=0)


def flat(block):
    return jnp.concatenate([block[i : i + 1] for i in range(4)], axis=1)


class Phase:
    def __init__(self):
        self.scope = None

    def __call__(self, name):
        if self.scope is not None:
            self.scope.__exit__(None, None, None)
        self.scope = None
        if name:
            self.scope = jax.named_scope(name)
            self.scope.__enter__()


class Ring:
    count = 33

    def __init__(self, net, buf, sems):
        self.net, self.buf = net, buf
        (self.ya_recv, self.ya_send, self.za_recv, self.za_send,
         self.zb_recv, self.zb_send, self.yb_recv, self.yb_send) = sems

    def a_y(self, zb, yb):
        return self.buf.at[zb * NY + yb, :, 0:CA]

    def a_z(self, zb, h):
        return self.buf.at[pl.ds(zb * NY + 2 * h, 2), :, 0:CA]

    def b(self, zb, yb):
        return self.buf.at[zb * NY + yb, :, CA:GU]

    def start_ya(self):
        n = self.net
        blk = self.a_y(n.z, n.y)
        for k in range(1, NY):
            n.send(blk, blk, self.ya_send.at[k], self.ya_recv.at[n.y], sp_1=(n.y + k) % NY)

    def finish_ya(self):
        n = self.net
        for k in range(1, NY):
            yk = (n.y + k) % NY
            n.arrived(self.a_y(n.z, yk), self.ya_send.at[k], self.ya_recv.at[yk], sp_1=yk)

    def forward_a(self, zb, chain, s, h):
        n = self.net
        blk = self.a_z(zb, h)
        n.send(blk, blk, self.za_send.at[(chain * HALF + s) * 2 + h], self.za_recv.at[zb * 2 + h],
               sp_0=n.zp if chain == 0 else n.zm)

    def forward_b(self, zb, chain, s):
        n = self.net
        blk = self.b(zb, n.y)
        n.send(blk, blk, self.zb_send.at[chain * HALF + s], self.zb_recv.at[zb],
               sp_0=n.zp if chain == 0 else n.zm)

    def start_yb(self, zb, o):
        n = self.net
        blk = self.b(zb, n.y)
        sem = self.yb_recv.at[zb * NY + n.y]
        n.send(blk, blk, self.yb_send.at[3 * o], sem, sp_1=n.yp)
        n.send(blk, blk, self.yb_send.at[3 * o + 1], sem, sp_1=n.ym)

    def own_a(self):
        self.finish_ya()
        for h in (0, 1):
            for chain in (0, 1):
                self.forward_a(self.net.z, chain, 0, h)

    def own_bz(self):
        for chain in (0, 1):
            self.forward_b(self.net.z, chain, 0)

    def own_by(self):
        self.start_yb(self.net.z, 0)

    def tick_a(self, s, h):
        n = self.net
        for chain in n.chains(s):
            zb = n.block(chain, s)
            n.arrived(self.a_z(zb, h), self.za_send.at[0], self.za_recv.at[zb * 2 + h], sp_0=n.zm)
            if n.goes_on(chain, s):
                self.forward_a(zb, chain, s, h)

    def tick_b(self, s):
        n = self.net
        for chain in n.chains(s):
            zb = n.block(chain, s)
            n.arrived(self.b(zb, n.y), self.zb_send.at[0], self.zb_recv.at[zb], sp_0=n.zm)
            if n.goes_on(chain, s):
                self.forward_b(zb, chain, s)
            self.start_yb(zb, n.order(chain, s))

    def tick_y(self, s):
        n = self.net
        for chain in n.chains(s):
            zb, o = n.block(chain, s), n.order(chain, s)
            blk = self.b(zb, n.ym)
            sem = self.yb_recv.at[zb * NY + n.ym]
            n.arrived(blk, self.yb_send.at[3 * o + 2], sem, sp_1=n.ym)
            n.send(blk, blk, self.yb_send.at[3 * o + 2], sem, sp_1=n.yp)

    def finish(self, s):
        n = self.net
        for chain in n.chains(s):
            zb, o = n.block(chain, s), n.order(chain, s)
            for yb in (n.yp, n.y2):
                n.arrived(self.b(zb, yb), self.yb_send.at[3 * o],
                          self.yb_recv.at[zb * NY + yb], sp_1=n.yp)


RING_SEMS = [NY, NY, 2 * NZ, 4 * HALF, NZ, NZ, NZ * NY, 3 * NZ]


class Pool:
    def __init__(self, net, buf, recv, ssem):
        self.net, self.buf, self.recv, self.ssem = net, buf, recv, ssem

    def at(self, b, h):
        return self.buf.at[b, :, h * (D // 2) : (h + 1) * (D // 2)]

    def put(self, b, h, k, to):
        blk = self.at(b, h)
        self.net.send(blk, blk, self.ssem.at[2 * k + h], self.recv.at[b * 2 + h], tp=to)

    def get(self, b, h, frm):
        self.net.arrived(self.at(b, h), self.ssem.at[0], self.recv.at[b * 2 + h], tp=frm)

    def start(self, h):
        n = self.net
        self.put(n.t, h, 0, n.tpp)
        self.put(n.t, h, 1, n.tpm)
        self.put(n.t, h, 2, n.tpo)

    def forward(self, h):
        n = self.net
        self.get(n.tpm, h, n.tpm)
        self.put(n.tpm, h, 3, n.tpp)
        self.put(n.tpm, h, 4, n.tpo)
        self.get(n.tpp, h, n.tpp)
        self.put(n.tpp, h, 5, n.tpo)

    def last(self, h):
        n = self.net
        self.get(n.tp2, h, n.tpm)
        self.put(n.tp2, h, 6, n.tpo)

    def finish(self, h):
        n = self.net
        for xb in (n.x, n.xp, n.xm, n.x2):
            self.get(xb * 2 + n.other, h, n.tpo)


class Net:
    def __init__(self):
        self.z = lax.axis_index("sp_0")
        self.y = lax.axis_index("sp_1")
        self.t = lax.axis_index("tp")
        z, y, t = self.z, self.y, self.t
        x, c = t // 2, t % 2
        self.x, self.c = x, c
        self.yp = (y + 1 + 2 * c) % NY
        self.ym = (y + 3 + 2 * c) % NY
        self.y2 = (y + 2) % NY
        self.zp = (z + 1 + (NZ - 2) * c) % NZ
        self.zm = (z + NZ - 1 + 2 * c) % NZ
        self.xp = (x + 1 + 2 * c) % NX
        self.xm = (x + 3 + 2 * c) % NX
        self.x2 = (x + 2) % NX
        self.other = 1 - c
        self.tpp = self.xp * 2 + c
        self.tpm = self.xm * 2 + c
        self.tp2 = self.x2 * 2 + c
        self.tpo = x * 2 + self.other
        self.sent = []

    def copy(self, src, dst, ss, rs, **dev):
        return pltpu.make_async_remote_copy(
            src_ref=src, dst_ref=dst, send_sem=ss, recv_sem=rs, device_id=dev, device_id_type=MESH
        )

    def send(self, src, dst, ss, rs, **dev):
        cp = self.copy(src, dst, ss, rs, **dev)
        cp.start()
        self.sent.append(cp)

    def arrived(self, dst, ss, rs, **dev):
        self.copy(dst, dst, ss, rs, **dev).wait_recv()

    def chains(self, s):
        return (0,) if s in (0, HALF) else (0, 1)

    def goes_on(self, chain, s):
        return s < (HALF if chain == 0 else HALF - 1)

    def block(self, chain, s):
        toward = self.zm - self.z if chain == 0 else self.zp - self.z
        return (self.z + NZ * NZ + s * toward) % NZ

    def order(self, chain, s):
        return 0 if s == 0 else 2 * s - 1 + chain


def kernel(
    x_in, dr_in, di_in, ls_in, inr_in, ini_in, our_in, oui_in, skip_in, op_in, gain_in,
    res_in, wg_in, wu_in, wd_in, keep_ref, out_ref,
    x_ref, dr_ref, di_ref, ls_ref, inr_ref, ini_ref, our_ref, oui_ref, skip_ref, gain_ref,
    res_ref, wg_ref, wu_ref, wd_ref,
    wgu, wdn, opall, sb, tb, act, acts, nf, hid, part, pr, ps, rs,
    ur, ui, mr, mi, er, ei, pcr, pci, carried, acc, *sems,
):
    net = Net()
    phase = Phase()
    z, y, t = net.z, net.y, net.t
    send, arrived = net.send, net.arrived
    gu = Ring(net, wgu, sems[0:8])
    dn = Ring(net, wdn, sems[8:16])
    (o_recv, o_send, n_recv, n_send, s_recv, s_send, t_recv, t_send, a_recv, a_send,
     p_recv, p_send, r_recv, r_send, in_sem) = sems[16:]
    pulls = [
        pltpu.make_async_copy(src, dst, in_sem.at[i])
        for i, (src, dst) in enumerate((
            (wg_in, wg_ref), (wu_in, wu_ref), (wd_in, wd_ref), (op_in, opall.at[t]),
            (dr_in, dr_ref), (di_in, di_ref), (ls_in, ls_ref), (x_in, x_ref),
            (inr_in, inr_ref), (ini_in, ini_ref), (our_in, our_ref), (oui_in, oui_ref),
            (skip_in, skip_ref), (gain_in, gain_ref), (res_in, res_ref),
        ))
    ]
    oproj = Pool(net, opall, o_recv, o_send)
    norms = Pool(net, nf, n_recv, n_send)

    phase("signal")
    barrier = pltpu.get_barrier_semaphore()
    for k in range(1, NZ):
        pl.semaphore_signal(barrier, inc=1, device_id={"sp_0": (z + k) % NZ}, device_id_type=MESH)
    for k in range(1, NY):
        pl.semaphore_signal(barrier, inc=1, device_id={"sp_1": (y + k) % NY}, device_id_type=MESH)
    for k in range(1, NT):
        pl.semaphore_signal(barrier, inc=1, device_id={"tp": (t + k) % NT}, device_id_type=MESH)

    phase("own")
    for pull in pulls:
        pull.start()
    for pull in pulls[:3]:
        pull.wait()
    own = z * NY + y
    wgu[own, :, 0:640] = wg_ref[:, 0:640]
    wgu[own, :, 640:1280] = wu_ref[:, 0:640]
    wgu[own, :, 1280:1408] = jnp.concatenate([wg_ref[:, 640:704], wu_ref[:, 640:704]], axis=1)
    wdn[own, :, 0:640] = wd_ref[0:16, 0:640]
    wdn[own, :, 640:1280] = wd_ref[16:32, 0:640]
    wdn[own, :, 1280:1408] = jnp.concatenate([wd_ref[0:16, 640:704], wd_ref[16:32, 640:704]], axis=1)
    pulls[3].wait()

    phase("barrier")
    pl.semaphore_wait(barrier, NT - 1 + NY - 1 + NZ - 1)

    phase("first_sends")
    gu.own_bz()
    gu.start_ya()
    oproj.start(0)
    oproj.start(1)
    gu.own_by()

    phase("coef")
    for pull in pulls[4:]:
        pull.wait()
    eight = lax.broadcasted_iota(jnp.int32, (8, 8), 0) == lax.broadcasted_iota(jnp.int32, (8, 8), 1)
    log_step = jnp.sum(
        jnp.where(eight, jnp.broadcast_to(ls_ref[...], (8, 8)), 0.0), axis=1, keepdims=True
    )
    a, ratio = discrete(dr_ref[...], di_ref[...], log_step)

    def line(v):
        return jnp.concatenate([v[g : g + 1] for g in range(8)], axis=1)

    a = (line(a[0]), line(a[1]))
    ratio = (line(ratio[0]), line(ratio[1]))
    powers = [a]
    for _ in range(7):
        powers.append(cmul(powers[-1], a))
    lift = tuple(jnp.concatenate([p[i] for p in powers], axis=0) for i in (0, 1))
    row8 = lax.broadcasted_iota(jnp.int32, (8, FL), 0)
    masked = []
    for k in (1, 2, 4):
        p = powers[k - 1]
        masked.append(tuple(jnp.where(row8 >= k, jnp.broadcast_to(v, (8, FL)), 0.0) for v in p))

    phase("drive")
    spread = (
        lax.broadcasted_iota(jnp.int32, (64, FL), 1) % 64
        == lax.broadcasted_iota(jnp.int32, (64, FL), 0)
    ).astype(F32).astype(BF16)
    block = (
        lax.broadcasted_iota(jnp.int32, (CHD, FL), 0) // 16
        == lax.broadcasted_iota(jnp.int32, (CHD, FL), 1) // 64
    )
    signal = x_ref[...]
    for src, dst in ((inr_ref, ur), (ini_ref, ui)):
        total = None
        for piece in pieces(src[...]):
            wide = jnp.where(block, dot(piece, spread), 0.0).astype(BF16)
            term = dot(signal, wide)
            total = term if total is None else total + term
        dst[...] = total

    phase("scan")

    def tile_step(i, carry):
        for j in range(4):
            rows = pl.ds(pl.multiple_of(i * 32 + j * 8, 8), 8)
            v = cmul(ratio, (ur[rows, :], ui[rows, :]))
            for k, m in zip((1, 2, 4), masked):
                v = cadd(v, cmul(m, (pltpu.roll(v[0], k, 0), pltpu.roll(v[1], k, 0))))
            ur[rows, :] = v[0]
            ui[rows, :] = v[1]
            er[pl.ds(i * 4 + j, 1), :] = v[0][7:8]
            ei[pl.ds(i * 4 + j, 1), :] = v[1][7:8]
        return carry

    lax.fori_loop(0, TOK // 32, tile_step, 0)

    phase("ends")
    row64 = lax.broadcasted_iota(jnp.int32, (64, FL), 0)
    e = (er[...], ei[...])
    ladder = []
    p = powers[7]
    for k in (1, 2, 4, 8, 16, 32):
        ladder.append(p)
        moved = tuple(jnp.where(row64 >= k, pltpu.roll(v, k, 0), 0.0) for v in e)
        e = cadd(e, cmul(p, moved))
        p = cmul(p, p)
    er[...] = e[0]
    ei[...] = e[1]
    a512 = (packed(p[0]), packed(p[1]))
    last = (e[0][63:64], e[1][63:64])
    sb[y, 0:4, :] = packed(last[0])
    sb[y, 4:8, :] = packed(last[1])
    for k in range(1, NY):
        send(sb.at[y], sb.at[y], s_send.at[k], s_recv.at[y], sp_1=(y + k) % NY)

    phase("lead")
    lead = (jnp.ones((64, FL), F32), jnp.zeros((64, FL), F32))
    for b, q in enumerate(ladder):
        more = cmul(q, lead)
        bit = (row64 // (1 << b)) % 2 == 1
        lead = tuple(jnp.where(bit, m, v) for m, v in zip(more, lead))
    pcr[...] = lead[0]
    pci[...] = lead[1]

    phase("outmat")
    for k, (src, sign) in enumerate(((our_ref, 1.0), (oui_ref, -1.0))):
        hi, lo = pieces(src[...] * sign)
        mr[k] = jnp.where(block, dot(hi, spread), 0.0).astype(BF16)
        mi[k] = jnp.where(block, dot(lo, spread), 0.0).astype(BF16)

    phase("b1")
    gu.tick_b(1)
    phase("own_a")
    gu.own_a()
    dn.start_ya()
    phase("b2")
    gu.tick_b(2)
    gu.tick_y(0)
    dn.own_bz()
    phase("s_wait")
    for k in range(1, NY):
        yk = (y + k) % NY
        arrived(sb.at[yk], s_send.at[k], s_recv.at[yk], sp_1=yk)
    whole = (jnp.zeros((4, 128), F32), jnp.zeros((4, 128), F32))
    before = whole
    ahead = (jnp.ones((4, 128), F32), jnp.zeros((4, 128), F32))
    for b in range(NY):
        own_b = (sb[b, 0:4, :], sb[b, 4:8, :])
        whole = cadd(cmul(a512, whole), own_b)
        inside = b < y
        step_b = cadd(cmul(a512, before), own_b)
        before = tuple(jnp.where(inside, n, v) for n, v in zip(step_b, before))
        step_a = cmul(a512, ahead)
        ahead = tuple(jnp.where(inside, n, v) for n, v in zip(step_a, ahead))
    a2 = cmul(a512, a512)
    a4 = cmul(a2, a2)
    tb[z, 0:4, :] = whole[0]
    tb[z, 4:8, :] = whole[1]
    for k in range(1, NZ):
        cp = net.copy(tb.at[z], tb.at[z], t_send.at[k], t_recv.at[z], sp_0=(z + k) % NZ)

        @pl.when(z + k < NZ)
        def _():
            cp.start()


    phase("a1")
    gu.tick_a(1, 0)
    phase("op0")
    oproj.forward(0)
    phase("a1b")
    gu.tick_a(1, 1)
    phase("b3")
    gu.tick_b(3)
    gu.tick_y(1)
    phase("op1")
    oproj.forward(1)
    phase("a2")
    gu.tick_a(2, 0)
    gu.tick_a(2, 1)
    dn.own_a()

    phase("t_wait")
    for b in range(NZ - 1):

        @pl.when(b < z)
        def _():
            arrived(tb.at[b], t_send.at[1], t_recv.at[b], sp_0=b)

    phase("hold")
    hold = (jnp.zeros((4, 128), F32), jnp.zeros((4, 128), F32))
    for b in range(NZ - 1):
        step_h = cadd(cmul(a4, hold), (tb[b, 0:4, :], tb[b, 4:8, :]))
        hold = tuple(jnp.where(b < z, n, v) for n, v in zip(step_h, hold))
    hold = cadd(cmul(ahead, hold), before)
    hold = (flat(hold[0]), flat(hold[1]))
    enter = cmul((pcr[...], pci[...]), hold)
    prev = tuple(jnp.where(row64 >= 1, pltpu.roll(v[...], 1, 0), 0.0) for v in (er, ei))
    enter = cadd(enter, prev)
    pcr[...] = enter[0]
    pci[...] = enter[1]

    phase("read")

    def read_step(i, carry):
        re, im = [], []
        for j in range(16):
            k = i * 16 + j
            rows = pl.ds(pl.multiple_of(k * 8, 8), 8)
            w = (pcr[pl.ds(k, 1), :], pci[pl.ds(k, 1), :])
            v = cadd((ur[rows, :], ui[rows, :]), cmul(lift, w))
            re.append(v[0])
            im.append(v[1])
        total = None
        for k, v in enumerate((re, im)):
            hi, lo = pieces(jnp.concatenate(v, axis=0))
            term = dot_t(hi, mr[k]) + dot_t(hi, mi[k]) + dot_t(lo, mr[k])
            total = term if total is None else total + term
        rows = pl.ds(pl.multiple_of(i * 128, 128), 128)
        pre = total + skip_ref[...] * x_ref[rows, :].astype(F32)
        inner = 0.7978845608028654 * (pre + 0.044715 * (pre * pre * pre))
        val = (pre * (0.5 * (1.0 + jnp.tanh(inner)))).astype(BF16)
        act[2 * i] = val[0:64]
        act[2 * i + 1] = val[64:128]
        return carry

    lax.fori_loop(0, 4, read_step, 0)
    for k in range(1, NT):
        tk = (t + k) % NT
        send(act.at[tk], acts.at[t], a_send.at[k], a_recv.at[t], tp=tk)
    acts[t] = act[t]

    phase("b4")
    gu.tick_b(4)
    phase("y2")
    gu.tick_y(2)
    dn.tick_b(1)
    phase("a3")
    gu.tick_a(3, 0)
    gu.tick_a(3, 1)
    phase("op_last")
    oproj.last(0)
    oproj.last(1)
    phase("b5")
    gu.tick_b(5)
    gu.tick_y(3)
    phase("d1")
    dn.tick_a(1, 0)
    dn.tick_a(1, 1)
    dn.own_by()
    phase("op_fin")
    oproj.finish(0)
    oproj.finish(1)

    phase("a_wait")
    for k in range(1, NT):
        tk = (t + k) % NT
        arrived(acts.at[tk], a_send.at[k], a_recv.at[tk], tp=tk)

    def near(o):
        s = (o + 1) // 2
        return (z + (NZ - s if o % 2 else s)) % NZ

    def up_dot(lo, hi, *cols):
        parts = []
        for c in cols:
            blocks = [wgu[pl.ds(near(o) * NY, NY), :, c : c + 128].reshape(128, 128) for o in range(lo, hi)]
            parts.append(jnp.concatenate(blocks, axis=0))
        w = parts[0] if len(parts) == 1 else jnp.concatenate(parts, axis=1)
        return dot(nf[:, :, lo * 128 : hi * 128].reshape(TOK, (hi - lo) * 128), w)

    def up_early(j):
        acc[:, j * 256 : (j + 1) * 256] = up_dot(0, EARLY, j * 128, 640 + j * 128)

    def up_step(j):
        v = acc[:, j * 256 : (j + 1) * 256] + up_dot(EARLY, NZ, j * 128, 640 + j * 128)
        g = v[:, 0:128]
        hid[:, j * 128 : (j + 1) * 128] = (g / (1.0 + jnp.exp(-g)) * v[:, 128:256]).astype(BF16)

    phase("mix")

    def mix_step(j, squares):
        cols = pl.ds(pl.multiple_of(j * 256, 256), 256)
        total = jnp.zeros((ROWS, 256), F32)
        for b in range(NT):
            total = total + dot(acts[b], opall[b, :, cols]).astype(BF16).astype(F32)
        v = res_ref[:, cols].astype(F32) + total.astype(BF16).astype(F32)
        carried[:, cols] = v
        return squares + jnp.sum(v * v, axis=1, keepdims=True)

    squares = lax.fori_loop(0, D // 512, mix_step, jnp.zeros((ROWS, 1), F32))
    gu.tick_a(4, 0)
    gu.tick_a(4, 1)
    dn.tick_b(2)
    squares = lax.fori_loop(D // 512, D // 256, mix_step, squares)
    scale = lax.rsqrt(squares * (1.0 / D) + 1e-06)
    for o in range(NZ):
        src = pl.ds(pl.multiple_of(near(o) * 128, 128), 128)
        nf[t, :, o * 128 : (o + 1) * 128] = (carried[:, src] * scale * gain_ref[:, src]).astype(BF16)
    keep = pltpu.make_async_copy(carried, keep_ref, in_sem.at[15])
    norms.start(0)
    norms.start(1)
    keep.start()
    phase("b6")
    gu.tick_b(6)
    gu.tick_y(4)
    phase("a5")
    gu.tick_a(5, 0)
    dn.tick_a(2, 0)
    gu.tick_a(5, 1)
    dn.tick_a(2, 1)
    phase("n0")
    norms.forward(0)
    phase("b7")
    gu.tick_b(7)
    gu.tick_y(5)
    dn.tick_b(3)
    dn.tick_y(0)
    phase("n1")
    norms.forward(1)
    phase("a6")
    gu.tick_a(6, 0)
    dn.tick_a(3, 0)
    gu.tick_a(6, 1)
    dn.tick_a(3, 1)
    norms.last(0)
    phase("b8")
    gu.tick_b(8)
    gu.tick_y(6)
    dn.tick_b(4)
    dn.tick_y(1)
    norms.last(1)
    phase("a7")
    gu.tick_a(7, 0)
    dn.tick_a(4, 0)
    gu.tick_a(7, 1)
    dn.tick_a(4, 1)
    gu.tick_y(7)
    dn.tick_b(5)
    dn.tick_y(2)
    gu.tick_y(8)
    phase("n_fin")
    norms.finish(0)
    norms.finish(1)
    for s in range(0, 7):
        gu.finish(s)
    phase("early0")
    up_early(0)
    up_early(1)
    phase("a8")
    gu.tick_a(8, 0)
    dn.tick_a(5, 0)
    phase("early1")
    up_early(2)
    phase("a8b")
    gu.tick_a(8, 1)
    dn.tick_a(5, 1)
    dn.tick_b(6)
    dn.tick_y(3)
    phase("early2")
    up_early(3)
    up_early(4)
    acc[:, 1280:1408] = up_dot(0, EARLY, 1280)
    phase("g_fin")
    for s in range(7, HALF + 1):
        gu.finish(s)

    phase("up0")
    for j in range(4):
        up_step(j)
    phase("d6")
    dn.tick_a(6, 0)
    dn.tick_a(6, 1)
    dn.tick_b(7)
    dn.tick_y(4)
    phase("up2")
    up_step(4)
    v = acc[:, 1280:1408] + up_dot(EARLY, NZ, 1280)
    v = v / (1.0 + jnp.exp(-v)) * pltpu.roll(v, 64, 1)
    low = lax.broadcasted_iota(jnp.int32, (TOK, 128), 1) < 64
    hid[:, 640:768] = jnp.where(low, v, 0.0).astype(BF16)

    def weights_of(zb):
        v = wdn[pl.ds(zb * NY, NY)]
        main = jnp.concatenate([v[:, :, 0:640], v[:, :, 640:1280]], axis=1).reshape(128, 640)
        tail = v[:, :, 1280:1408]
        turned = pltpu.roll(tail.reshape(64, 128).astype(F32), 64, 1).astype(BF16)
        tail = jnp.concatenate([tail, turned.reshape(NY, 16, 128)], axis=1).reshape(128, 128)
        return jnp.concatenate([main, tail], axis=1)

    def place(o):
        s = o // 2 + 1
        if s == HALF:
            return (z + HALF * (o % 2)) % NZ
        return (z + (s if o % 2 else NZ - s)) % NZ

    def down_step(i):
        w = jnp.concatenate([weights_of(place(2 * i)), weights_of(place(2 * i + 1))], axis=0)
        v = dot_t(hid[...], w)
        part[:, :, i * 256 : (i + 1) * 256] = v.astype(BF16).reshape(NT, ROWS, 256)

    xs = (net.x2, net.xm, net.xp, net.x)

    def span(k):
        return pl.ds(SPANS[k][0] * 256, (SPANS[k][1] - SPANS[k][0]) * 256)

    def sum_start(k):
        for i, xb in enumerate(xs):
            send(part.at[xb * 2 + net.other, :, span(k)], pr.at[xb, :, span(k)],
                 p_send.at[4 * k + i], p_recv.at[NX * k + xb], tp=net.tpo)

    def pair(k, xb):
        arrived(pr.at[xb, :, span(k)], p_send.at[0], p_recv.at[NX * k + xb], tp=net.tpo)
        mine = part[xb * 2 + net.c, :, span(k)].astype(F32)
        return mine + pr[xb, :, span(k)].astype(F32)

    def hop(k, i, value, to):
        ps[i, :, span(k)] = value.astype(BF16)
        send(ps.at[i, :, span(k)], rs.at[i, :, span(k)],
             r_send.at[3 * k + i], r_recv.at[3 * k + i], tp=to)

    def landed(k, i, frm):
        arrived(rs.at[i, :, span(k)], r_send.at[0], r_recv.at[3 * k + i], tp=frm)
        return rs[i, :, span(k)].astype(F32)

    def sum_pair(k):
        hop(k, 0, pair(k, net.x2), net.tp2 if k >= STRAIGHT else net.tpp)
        hop(k, 1, pair(k, net.xm), net.tpm)
        if k >= STRAIGHT:
            hop(k, 2, pair(k, net.xp), net.tpp)

    def sum_relay(k):
        if k >= STRAIGHT:
            return
        near = pair(k, net.xp)
        hop(k, 2, near + landed(k, 0, net.tpm), net.tpp)

    def sum_finish(k):
        total = pair(k, net.x) + landed(k, 1, net.tpp) + landed(k, 2, net.tpm)
        if k >= STRAIGHT:
            total = total + landed(k, 0, net.tp2)
        total = total.astype(BF16)
        for i in range(2 * (SPANS[k][1] - SPANS[k][0])):
            cols = pl.ds(pl.multiple_of(place(2 * SPANS[k][0] + i) * 128, 128), 128)
            out_ref[:, cols] = total[:, i * 128 : (i + 1) * 128]

    phase("w0")
    dn.finish(1)
    down_step(0)
    dn.finish(2)
    down_step(1)
    sum_start(0)
    phase("d7")
    dn.tick_a(7, 0)
    dn.tick_a(7, 1)
    dn.tick_b(8)
    dn.tick_y(5)
    dn.tick_y(6)
    phase("w2")
    dn.finish(3)
    down_step(2)
    sum_pair(0)
    dn.finish(4)
    down_step(3)
    sum_start(1)
    phase("d8")
    dn.tick_a(8, 0)
    dn.tick_a(8, 1)
    dn.tick_y(7)
    dn.tick_y(8)
    phase("w4")
    dn.finish(5)
    down_step(4)
    sum_pair(1)
    phase("w5")
    dn.finish(6)
    down_step(5)
    sum_start(2)
    sum_relay(0)
    phase("w6")
    dn.finish(7)
    down_step(6)
    sum_pair(2)
    phase("w7")
    dn.finish(0)
    dn.finish(8)
    down_step(7)
    sum_start(3)
    phase("relay1")
    sum_relay(1)
    sum_pair(3)
    phase("rs0")
    sum_relay(2)
    sum_finish(0)
    phase("rs1")
    sum_finish(1)
    phase("rs2")
    sum_finish(2)
    phase("rs3")
    sum_finish(3)

    phase("drain")
    keep.wait()
    for cp in net.sent:
        cp.wait_send()
    for k in range(1, NZ):

        @pl.when(z + k < NZ)
        def _():
            net.copy(tb.at[z], tb.at[z], t_send.at[k], t_recv.at[z], sp_0=(z + k) % NZ).wait_send()

    phase(None)


def on_device(
    mixer_in, residual, decay_real, decay_imag, log_step, in_real, in_imag,
    output_real, output_imaginary, skip, out_proj, norm_gain, w_gate, w_up, w_down,
):
    vmem = pltpu.VMEM
    dma = pltpu.SemaphoreType.DMA
    scratch = [
        vmem((TOK, CHD), BF16),
        vmem((8, 64), F32),
        vmem((8, 64), F32),
        vmem((1, 8), F32),
        vmem((CHD, 64), F32),
        vmem((CHD, 64), F32),
        vmem((CHD, 64), F32),
        vmem((CHD, 64), F32),
        vmem((1, CHD), F32),
        vmem((1, D), F32),
        vmem((ROWS, D), BF16),
        vmem((32, FFD), BF16),
        vmem((32, FFD), BF16),
        vmem((32, FFD), BF16),
        vmem((NZ * NY, 32, GU), BF16),
        vmem((NZ * NY, 16, GU), BF16),
        vmem((NT, CHD, D), BF16),
        vmem((NY, 8, 128), F32),
        vmem((NZ, 8, 128), F32),
        vmem((NT, ROWS, CHD), BF16),
        vmem((NT, ROWS, CHD), BF16),
        vmem((NT, ROWS, D), BF16),
        vmem((TOK, 768), BF16),
        vmem((NT, ROWS, D), BF16),
        vmem((NX, ROWS, D), BF16),
        vmem((3, ROWS, D), BF16),
        vmem((3, ROWS, D), BF16),
        vmem((TOK, FL), F32),
        vmem((TOK, FL), F32),
        vmem((2, CHD, FL), BF16),
        vmem((2, CHD, FL), BF16),
        vmem((64, FL), F32),
        vmem((64, FL), F32),
        vmem((64, FL), F32),
        vmem((64, FL), F32),
        vmem((ROWS, D), F32),
        vmem((TOK, GU), F32),
    ]
    counts = RING_SEMS + RING_SEMS + [
        2 * NT, 14, 2 * NT, 14, NY, NY, NZ, NZ, NT, NT, NC * NX, NC * 4, NC * 3, NC * 3, 16,
    ]
    scratch += [dma((n,)) for n in counts]
    carried, down = pl.pallas_call(
        kernel,
        out_shape=(jax.ShapeDtypeStruct((ROWS, D), F32), jax.ShapeDtypeStruct((ROWS, D), BF16)),
        in_specs=[pl.BlockSpec(memory_space=pl.ANY)] * 15,
        out_specs=(pl.BlockSpec(memory_space=pl.ANY), pl.BlockSpec(memory_space=vmem)),
        scratch_shapes=scratch,
        compiler_params=pltpu.CompilerParams(
            collective_id=0, has_side_effects=True, vmem_limit_bytes=60 * 1024 * 1024
        ),
    )(
        mixer_in, decay_real, decay_imag, log_step.reshape(1, 8),
        jnp.transpose(in_real, (0, 2, 1)).reshape(CHD, 64),
        jnp.transpose(in_imag, (0, 2, 1)).reshape(CHD, 64),
        output_real.reshape(CHD, 64), output_imaginary.reshape(CHD, 64),
        skip.reshape(1, CHD), out_proj, norm_gain.reshape(1, D),
        residual, w_gate, w_up, w_down.T,
    )
    return (carried + 0.5 * down.astype(F32)).astype(BF16)


def solution(mesh):
    finer = Mesh(mesh.devices.reshape(NZ, NY, mesh.shape["tp"]), ("sp_0", "sp_1", "tp"))
    return jax.shard_map(
        on_device,
        mesh=finer,
        in_specs=(
            P(SP, "tp"),
            P(SP_TP, None),
            P("tp", None),
            P("tp", None),
            P("tp"),
            P("tp", None, None),
            P("tp", None, None),
            P("tp", None, None),
            P("tp", None, None),
            P("tp"),
            P("tp", None),
            P(),
            P(SP, "tp"),
            P(SP, "tp"),
            P("tp", SP),
        ),
        out_specs=P(SP_TP, None),
        check_vma=False,
    )
```

```python
import functools

import jax
import jax.numpy as jnp
from jax import lax
from jax.experimental import pallas as pl
from jax.experimental.pallas import tpu as pltpu
from jax.sharding import Mesh
from jax.sharding import PartitionSpec as P

SP = ("sp_0", "sp_1")
SP_TP = ("sp_0", "sp_1", "tp")
MESH = pl.DeviceIdType.MESH
F32 = jnp.float32
BF16 = jnp.bfloat16

NZ = 16
NY = 4
NX = 4
NT = 8
HALF = NZ // 2
EARLY = 12
D = 2048
TOK = 512
ROWS = TOK // NT
FL = 512
CHD = 128
FFD = 704
GU = 2 * FFD
CA = 512
CD = 384
SPANS = ((0, 2), (2, 4), (4, 6), (6, 8))
NC = len(SPANS)
STRAIGHT = 2


def discrete(decay_real, decay_imag, log_step):
    step_size = jnp.exp(log_step)
    magnitude = jnp.exp(decay_real * step_size)
    angle = decay_imag * step_size
    power_re = magnitude * jnp.cos(angle)
    power_im = magnitude * jnp.sin(angle)
    denom = decay_real * decay_real + decay_imag * decay_imag
    ratio_re = ((power_re - 1.0) * decay_real + power_im * decay_imag) / denom
    ratio_im = (power_im * decay_real - (power_re - 1.0) * decay_imag) / denom
    return (power_re, power_im), (ratio_re, ratio_im)


def cmul(a, b):
    return (a[0] * b[0] - a[1] * b[1], a[0] * b[1] + a[1] * b[0])


def cadd(a, b):
    return (a[0] + b[0], a[1] + b[1])


def pieces(v):
    hi = v.astype(BF16)
    lo = (v - hi.astype(F32)).astype(BF16)
    return hi, lo


def dot(a, b):
    return jnp.dot(a, b, preferred_element_type=F32)


def dot_t(a, b):
    return lax.dot_general(a, b, (((1,), (1,)), ((), ())), preferred_element_type=F32)


def packed(row):
    return jnp.concatenate([row[:, i * 128 : (i + 1) * 128] for i in range(4)], axis=0)


def flat(block):
    return jnp.concatenate([block[i : i + 1] for i in range(4)], axis=1)


class Phase:
    def __init__(self):
        self.scope = None

    def __call__(self, name):
        if self.scope is not None:
            self.scope.__exit__(None, None, None)
        self.scope = None
        if name:
            self.scope = jax.named_scope(name)
            self.scope.__enter__()


class Ring:
    count = 33

    def __init__(self, net, buf, ca, sems):
        self.net, self.buf, self.ca = net, buf, ca
        (self.ya_recv, self.ya_send, self.za_recv, self.za_send,
         self.zb_recv, self.zb_send, self.yb_recv, self.yb_send) = sems

    def a_y(self, zb, yb):
        return self.buf.at[zb * NY + yb, :, 0 : self.ca]

    def a_z(self, zb, h):
        return self.buf.at[pl.ds(zb * NY + 2 * h, 2), :, 0 : self.ca]

    def b(self, zb, yb):
        return self.buf.at[zb * NY + yb, :, self.ca : GU]

    def start_ya(self):
        n = self.net
        blk = self.a_y(n.z, n.y)
        for k in range(1, NY):
            n.send(blk, blk, self.ya_send.at[k], self.ya_recv.at[n.y], sp_1=(n.y + k) % NY)

    def finish_ya(self):
        n = self.net
        for k in range(1, NY):
            yk = (n.y + k) % NY
            n.arrived(self.a_y(n.z, yk), self.ya_send.at[k], self.ya_recv.at[yk], sp_1=yk)

    def forward_a(self, zb, chain, s, h):
        n = self.net
        blk = self.a_z(zb, h)
        n.send(blk, blk, self.za_send.at[(chain * HALF + s) * 2 + h], self.za_recv.at[zb * 2 + h],
               sp_0=n.zp if chain == 0 else n.zm)

    def forward_b(self, zb, chain, s):
        n = self.net
        blk = self.b(zb, n.y)
        n.send(blk, blk, self.zb_send.at[chain * HALF + s], self.zb_recv.at[zb],
               sp_0=n.zp if chain == 0 else n.zm)

    def start_yb(self, zb, o):
        n = self.net
        blk = self.b(zb, n.y)
        sem = self.yb_recv.at[zb * NY + n.y]
        n.send(blk, blk, self.yb_send.at[3 * o], sem, sp_1=n.yp)
        n.send(blk, blk, self.yb_send.at[3 * o + 1], sem, sp_1=n.ym)

    def own_a(self):
        self.finish_ya()
        for h in (0, 1):
            for chain in (0, 1):
                self.forward_a(self.net.z, chain, 0, h)

    def own_bz(self):
        for chain in (0, 1):
            self.forward_b(self.net.z, chain, 0)

    def own_by(self):
        self.start_yb(self.net.z, 0)

    def tick_a(self, s, h):
        n = self.net
        for chain in n.chains(s):
            zb = n.block(chain, s)
            n.arrived(self.a_z(zb, h), self.za_send.at[0], self.za_recv.at[zb * 2 + h], sp_0=n.zm)
            if n.goes_on(chain, s):
                self.forward_a(zb, chain, s, h)

    def start_y(self, s):
        n = self.net
        for chain in n.chains(s):
            self.start_yb(n.block(chain, s), n.order(chain, s))

    def tick_b(self, s, along_y=True):
        n = self.net
        for chain in n.chains(s):
            zb = n.block(chain, s)
            n.arrived(self.b(zb, n.y), self.zb_send.at[0], self.zb_recv.at[zb], sp_0=n.zm)
            if n.goes_on(chain, s):
                self.forward_b(zb, chain, s)
            if along_y:
                self.start_yb(zb, n.order(chain, s))

    def tick_y(self, s):
        n = self.net
        for chain in n.chains(s):
            zb, o = n.block(chain, s), n.order(chain, s)
            blk = self.b(zb, n.ym)
            sem = self.yb_recv.at[zb * NY + n.ym]
            n.arrived(blk, self.yb_send.at[3 * o + 2], sem, sp_1=n.ym)
            n.send(blk, blk, self.yb_send.at[3 * o + 2], sem, sp_1=n.yp)

    def finish(self, s):
        n = self.net
        for chain in n.chains(s):
            zb, o = n.block(chain, s), n.order(chain, s)
            for yb in (n.yp, n.y2):
                n.arrived(self.b(zb, yb), self.yb_send.at[3 * o],
                          self.yb_recv.at[zb * NY + yb], sp_1=n.yp)


RING_SEMS = [NY, NY, 2 * NZ, 4 * HALF, NZ, NZ, NZ * NY, 3 * NZ]


class Pool:
    def __init__(self, net, buf, recv, ssem):
        self.net, self.buf, self.recv, self.ssem = net, buf, recv, ssem

    def at(self, b, h):
        return self.buf.at[b, :, h * (D // 2) : (h + 1) * (D // 2)]

    def put(self, b, h, k, to):
        blk = self.at(b, h)
        self.net.send(blk, blk, self.ssem.at[2 * k + h], self.recv.at[b * 2 + h], tp=to)

    def get(self, b, h, frm):
        self.net.arrived(self.at(b, h), self.ssem.at[0], self.recv.at[b * 2 + h], tp=frm)

    def start(self, h):
        n = self.net
        self.put(n.t, h, 0, n.tpp)
        self.put(n.t, h, 1, n.tpm)
        self.put(n.t, h, 2, n.tpo)

    def forward(self, h):
        n = self.net
        self.get(n.tpm, h, n.tpm)
        self.put(n.tpm, h, 3, n.tpp)
        self.put(n.tpm, h, 4, n.tpo)
        self.get(n.tpp, h, n.tpp)
        self.put(n.tpp, h, 5, n.tpo)

    def last(self, h):
        n = self.net
        self.get(n.tp2, h, n.tpm)
        self.put(n.tp2, h, 6, n.tpo)

    def finish(self, h):
        n = self.net
        for xb in (n.x, n.xp, n.xm, n.x2):
            self.get(xb * 2 + n.other, h, n.tpo)


class Net:
    def __init__(self):
        self.z = lax.axis_index("sp_0")
        self.y = lax.axis_index("sp_1")
        self.t = lax.axis_index("tp")
        z, y, t = self.z, self.y, self.t
        x, c = t // 2, t % 2
        self.x, self.c = x, c
        self.yp = (y + 1 + 2 * c) % NY
        self.ym = (y + 3 + 2 * c) % NY
        self.y2 = (y + 2) % NY
        self.zp = (z + 1 + (NZ - 2) * c) % NZ
        self.zm = (z + NZ - 1 + 2 * c) % NZ
        self.xp = (x + 1 + 2 * c) % NX
        self.xm = (x + 3 + 2 * c) % NX
        self.x2 = (x + 2) % NX
        self.other = 1 - c
        self.tpp = self.xp * 2 + c
        self.tpm = self.xm * 2 + c
        self.tp2 = self.x2 * 2 + c
        self.tpo = x * 2 + self.other
        self.sent = []

    def copy(self, src, dst, ss, rs, **dev):
        return pltpu.make_async_remote_copy(
            src_ref=src, dst_ref=dst, send_sem=ss, recv_sem=rs, device_id=dev, device_id_type=MESH
        )

    def send(self, src, dst, ss, rs, **dev):
        cp = self.copy(src, dst, ss, rs, **dev)
        cp.start()
        self.sent.append(cp)

    def arrived(self, dst, ss, rs, **dev):
        self.copy(dst, dst, ss, rs, **dev).wait_recv()

    def chains(self, s):
        return (0,) if s in (0, HALF) else (0, 1)

    def goes_on(self, chain, s):
        return s < (HALF if chain == 0 else HALF - 1)

    def block(self, chain, s):
        toward = self.zm - self.z if chain == 0 else self.zp - self.z
        return (self.z + NZ * NZ + s * toward) % NZ

    def order(self, chain, s):
        return 0 if s == 0 else 2 * s - 1 + chain


def kernel(
    x_in, dr_in, di_in, ls_in, inr_in, ini_in, our_in, oui_in, skip_in, op_in, gain_in,
    res_in, wg_in, wu_in, wd_in, keep_ref, out_ref,
    x_ref, dr_ref, di_ref, ls_ref, inr_ref, ini_ref, our_ref, oui_ref, skip_ref, gain_ref,
    res_ref, wg_ref, wu_ref, wd_ref,
    wgu, wdn, opall, sb, tb, act, acts, nf, hid, part, pr, ps, rs,
    ur, ui, mr, mi, er, ei, pcr, pci, carried, acc, *sems,
):
    net = Net()
    phase = Phase()
    z, y, t = net.z, net.y, net.t
    send, arrived = net.send, net.arrived
    gu = Ring(net, wgu, CA, sems[0:8])
    dn = Ring(net, wdn, CD, sems[8:16])
    (o_recv, o_send, n_recv, n_send, s_recv, s_send, t_recv, t_send, a_recv, a_send,
     p_recv, p_send, r_recv, r_send, in_sem) = sems[16:]
    pulls = [
        pltpu.make_async_copy(src, dst, in_sem.at[i])
        for i, (src, dst) in enumerate((
            (wg_in, wg_ref), (wu_in, wu_ref), (wd_in, wd_ref), (op_in, opall.at[t]),
            (dr_in, dr_ref), (di_in, di_ref), (ls_in, ls_ref), (x_in, x_ref),
            (inr_in, inr_ref), (ini_in, ini_ref), (our_in, our_ref), (oui_in, oui_ref),
            (skip_in, skip_ref), (gain_in, gain_ref), (res_in, res_ref),
        ))
    ]
    oproj = Pool(net, opall, o_recv, o_send)
    norms = Pool(net, nf, n_recv, n_send)

    phase("signal")
    barrier = pltpu.get_barrier_semaphore()
    for k in range(1, NZ):
        pl.semaphore_signal(barrier, inc=1, device_id={"sp_0": (z + k) % NZ}, device_id_type=MESH)
    for k in range(1, NY):
        pl.semaphore_signal(barrier, inc=1, device_id={"sp_1": (y + k) % NY}, device_id_type=MESH)
    for k in range(1, NT):
        pl.semaphore_signal(barrier, inc=1, device_id={"tp": (t + k) % NT}, device_id_type=MESH)

    phase("own")
    for pull in pulls:
        pull.start()
    for pull in pulls[:3]:
        pull.wait()
    own = z * NY + y
    wgu[own, :, 0:640] = wg_ref[:, 0:640]
    wgu[own, :, 640:1280] = wu_ref[:, 0:640]
    wgu[own, :, 1280:1408] = jnp.concatenate([wg_ref[:, 640:704], wu_ref[:, 640:704]], axis=1)
    wdn[own, :, 0:640] = wd_ref[0:16, 0:640]
    wdn[own, :, 640:1280] = wd_ref[16:32, 0:640]
    wdn[own, :, 1280:1408] = jnp.concatenate([wd_ref[0:16, 640:704], wd_ref[16:32, 640:704]], axis=1)
    pulls[3].wait()

    phase("barrier")
    pl.semaphore_wait(barrier, NT - 1 + NY - 1 + NZ - 1)

    phase("first_sends")
    gu.own_bz()
    gu.start_ya()
    oproj.start(0)
    oproj.start(1)
    gu.own_by()

    phase("coef")
    for pull in pulls[4:]:
        pull.wait()
    eight = lax.broadcasted_iota(jnp.int32, (8, 8), 0) == lax.broadcasted_iota(jnp.int32, (8, 8), 1)
    log_step = jnp.sum(
        jnp.where(eight, jnp.broadcast_to(ls_ref[...], (8, 8)), 0.0), axis=1, keepdims=True
    )
    a, ratio = discrete(dr_ref[...], di_ref[...], log_step)

    def line(v):
        return jnp.concatenate([v[g : g + 1] for g in range(8)], axis=1)

    a = (line(a[0]), line(a[1]))
    ratio = (line(ratio[0]), line(ratio[1]))
    powers = [a]
    for _ in range(7):
        powers.append(cmul(powers[-1], a))
    lift = tuple(jnp.concatenate([p[i] for p in powers], axis=0) for i in (0, 1))
    row8 = lax.broadcasted_iota(jnp.int32, (8, FL), 0)
    masked = []
    for k in (1, 2, 4):
        p = powers[k - 1]
        masked.append(tuple(jnp.where(row8 >= k, jnp.broadcast_to(v, (8, FL)), 0.0) for v in p))

    phase("drive")
    spread = (
        lax.broadcasted_iota(jnp.int32, (64, FL), 1) % 64
        == lax.broadcasted_iota(jnp.int32, (64, FL), 0)
    ).astype(F32).astype(BF16)
    block = (
        lax.broadcasted_iota(jnp.int32, (CHD, FL), 0) // 16
        == lax.broadcasted_iota(jnp.int32, (CHD, FL), 1) // 64
    )
    signal = x_ref[...]
    for src, dst in ((inr_ref, ur), (ini_ref, ui)):
        total = None
        for piece in pieces(src[...]):
            wide = jnp.where(block, dot(piece, spread), 0.0).astype(BF16)
            term = dot(signal, wide)
            total = term if total is None else total + term
        dst[...] = total

    phase("scan")

    def tile_step(i, carry):
        for j in range(4):
            rows = pl.ds(pl.multiple_of(i * 32 + j * 8, 8), 8)
            v = cmul(ratio, (ur[rows, :], ui[rows, :]))
            for k, m in zip((1, 2, 4), masked):
                v = cadd(v, cmul(m, (pltpu.roll(v[0], k, 0), pltpu.roll(v[1], k, 0))))
            ur[rows, :] = v[0]
            ui[rows, :] = v[1]
            er[pl.ds(i * 4 + j, 1), :] = v[0][7:8]
            ei[pl.ds(i * 4 + j, 1), :] = v[1][7:8]
        return carry

    lax.fori_loop(0, TOK // 32, tile_step, 0)

    phase("ends")
    row64 = lax.broadcasted_iota(jnp.int32, (64, FL), 0)
    e = (er[...], ei[...])
    ladder = []
    p = powers[7]
    for k in (1, 2, 4, 8, 16, 32):
        ladder.append(p)
        moved = tuple(jnp.where(row64 >= k, pltpu.roll(v, k, 0), 0.0) for v in e)
        e = cadd(e, cmul(p, moved))
        p = cmul(p, p)
    er[...] = e[0]
    ei[...] = e[1]
    a512 = (packed(p[0]), packed(p[1]))
    last = (e[0][63:64], e[1][63:64])
    sb[y, 0:4, :] = packed(last[0])
    sb[y, 4:8, :] = packed(last[1])
    for k in range(1, NY):
        send(sb.at[y], sb.at[y], s_send.at[k], s_recv.at[y], sp_1=(y + k) % NY)

    phase("lead")
    lead = (jnp.ones((64, FL), F32), jnp.zeros((64, FL), F32))
    for b, q in enumerate(ladder):
        more = cmul(q, lead)
        bit = (row64 // (1 << b)) % 2 == 1
        lead = tuple(jnp.where(bit, m, v) for m, v in zip(more, lead))
    pcr[...] = lead[0]
    pci[...] = lead[1]

    phase("outmat")
    for k, (src, sign) in enumerate(((our_ref, 1.0), (oui_ref, -1.0))):
        hi, lo = pieces(src[...] * sign)
        mr[k] = jnp.where(block, dot(hi, spread), 0.0).astype(BF16)
        mi[k] = jnp.where(block, dot(lo, spread), 0.0).astype(BF16)

    phase("b1")
    gu.tick_b(1)
    phase("own_a")
    gu.own_a()
    dn.start_ya()
    phase("b2")
    gu.tick_b(2)
    gu.tick_y(0)
    dn.own_bz()
    phase("s_wait")
    for k in range(1, NY):
        yk = (y + k) % NY
        arrived(sb.at[yk], s_send.at[k], s_recv.at[yk], sp_1=yk)
    whole = (jnp.zeros((4, 128), F32), jnp.zeros((4, 128), F32))
    before = whole
    ahead = (jnp.ones((4, 128), F32), jnp.zeros((4, 128), F32))
    for b in range(NY):
        own_b = (sb[b, 0:4, :], sb[b, 4:8, :])
        whole = cadd(cmul(a512, whole), own_b)
        inside = b < y
        step_b = cadd(cmul(a512, before), own_b)
        before = tuple(jnp.where(inside, n, v) for n, v in zip(step_b, before))
        step_a = cmul(a512, ahead)
        ahead = tuple(jnp.where(inside, n, v) for n, v in zip(step_a, ahead))
    a2 = cmul(a512, a512)
    a4 = cmul(a2, a2)
    tb[z, 0:4, :] = whole[0]
    tb[z, 4:8, :] = whole[1]
    for k in range(1, NZ):
        cp = net.copy(tb.at[z], tb.at[z], t_send.at[k], t_recv.at[z], sp_0=(z + k) % NZ)

        @pl.when(z + k < NZ)
        def _():
            cp.start()


    phase("a1")
    gu.tick_a(1, 0)
    phase("op0")
    oproj.forward(0)
    phase("a1b")
    gu.tick_a(1, 1)
    phase("b3")
    gu.tick_b(3)
    gu.tick_y(1)
    phase("op1")
    oproj.forward(1)
    phase("a2")
    gu.tick_a(2, 0)
    gu.tick_a(2, 1)
    dn.own_a()

    phase("t_wait")
    for b in range(NZ - 1):

        @pl.when(b < z)
        def _():
            arrived(tb.at[b], t_send.at[1], t_recv.at[b], sp_0=b)

    phase("hold")
    hold = (jnp.zeros((4, 128), F32), jnp.zeros((4, 128), F32))
    for b in range(NZ - 1):
        step_h = cadd(cmul(a4, hold), (tb[b, 0:4, :], tb[b, 4:8, :]))
        hold = tuple(jnp.where(b < z, n, v) for n, v in zip(step_h, hold))
    hold = cadd(cmul(ahead, hold), before)
    hold = (flat(hold[0]), flat(hold[1]))
    enter = cmul((pcr[...], pci[...]), hold)
    prev = tuple(jnp.where(row64 >= 1, pltpu.roll(v[...], 1, 0), 0.0) for v in (er, ei))
    enter = cadd(enter, prev)
    pcr[...] = enter[0]
    pci[...] = enter[1]

    phase("read")

    def read_step(i, carry):
        re, im = [], []
        for j in range(16):
            k = i * 16 + j
            rows = pl.ds(pl.multiple_of(k * 8, 8), 8)
            w = (pcr[pl.ds(k, 1), :], pci[pl.ds(k, 1), :])
            v = cadd((ur[rows, :], ui[rows, :]), cmul(lift, w))
            re.append(v[0])
            im.append(v[1])
        total = None
        for k, v in enumerate((re, im)):
            hi, lo = pieces(jnp.concatenate(v, axis=0))
            term = dot_t(hi, mr[k]) + dot_t(hi, mi[k]) + dot_t(lo, mr[k])
            total = term if total is None else total + term
        rows = pl.ds(pl.multiple_of(i * 128, 128), 128)
        pre = total + skip_ref[...] * x_ref[rows, :].astype(F32)
        inner = 0.7978845608028654 * (pre + 0.044715 * (pre * pre * pre))
        val = (pre * (0.5 * (1.0 + jnp.tanh(inner)))).astype(BF16)
        act[2 * i] = val[0:64]
        act[2 * i + 1] = val[64:128]
        return carry

    lax.fori_loop(0, 4, read_step, 0)
    for k in range(1, NT):
        tk = (t + k) % NT
        send(act.at[tk], acts.at[t], a_send.at[k], a_recv.at[t], tp=tk)
    acts[t] = act[t]

    phase("b4")
    gu.tick_b(4)
    phase("y2")
    gu.tick_y(2)
    dn.tick_b(1)
    phase("a3")
    gu.tick_a(3, 0)
    gu.tick_a(3, 1)
    phase("op_last")
    oproj.last(0)
    oproj.last(1)
    phase("b5")
    gu.tick_b(5)
    gu.tick_y(3)
    phase("d1")
    dn.tick_a(1, 0)
    dn.tick_a(1, 1)
    dn.own_by()
    phase("op_fin")
    oproj.finish(0)
    oproj.finish(1)

    phase("a_wait")
    for k in range(1, NT):
        tk = (t + k) % NT
        arrived(acts.at[tk], a_send.at[k], a_recv.at[tk], tp=tk)

    def near(o):
        s = (o + 1) // 2
        return (z + (NZ - s if o % 2 else s)) % NZ

    def up_dot(lo, hi, *cols):
        parts = []
        for c in cols:
            blocks = [wgu[pl.ds(near(o) * NY, NY), :, c : c + 128].reshape(128, 128) for o in range(lo, hi)]
            parts.append(jnp.concatenate(blocks, axis=0))
        w = parts[0] if len(parts) == 1 else jnp.concatenate(parts, axis=1)
        return dot(nf[:, :, lo * 128 : hi * 128].reshape(TOK, (hi - lo) * 128), w)

    def up_early(j):
        acc[:, j * 256 : (j + 1) * 256] = up_dot(0, EARLY, j * 128, 640 + j * 128)

    def up_step(j):
        v = acc[:, j * 256 : (j + 1) * 256] + up_dot(EARLY, NZ, j * 128, 640 + j * 128)
        g = v[:, 0:128]
        hid[:, j * 128 : (j + 1) * 128] = (g / (1.0 + jnp.exp(-g)) * v[:, 128:256]).astype(BF16)

    phase("mix")

    def mix_step(j, squares):
        cols = pl.ds(pl.multiple_of(j * 256, 256), 256)
        total = jnp.zeros((ROWS, 256), F32)
        for b in range(NT):
            total = total + dot(acts[b], opall[b, :, cols]).astype(BF16).astype(F32)
        v = res_ref[:, cols].astype(F32) + total.astype(BF16).astype(F32)
        carried[:, cols] = v
        return squares + jnp.sum(v * v, axis=1, keepdims=True)

    squares = lax.fori_loop(0, D // 512, mix_step, jnp.zeros((ROWS, 1), F32))
    gu.tick_a(4, 0)
    gu.tick_a(4, 1)
    dn.tick_b(2)
    squares = lax.fori_loop(D // 512, D // 256, mix_step, squares)
    scale = lax.rsqrt(squares * (1.0 / D) + 1e-06)
    for o in range(NZ):
        src = pl.ds(pl.multiple_of(near(o) * 128, 128), 128)
        nf[t, :, o * 128 : (o + 1) * 128] = (carried[:, src] * scale * gain_ref[:, src]).astype(BF16)
    keep = pltpu.make_async_copy(carried, keep_ref, in_sem.at[15])
    norms.start(0)
    norms.start(1)
    keep.start()
    phase("b6")
    gu.tick_b(6)
    gu.tick_y(4)
    phase("a5")
    gu.tick_a(5, 0)
    dn.tick_a(2, 0)
    gu.tick_a(5, 1)
    dn.tick_a(2, 1)
    phase("n0")
    norms.forward(0)
    phase("b7")
    gu.tick_b(7)
    gu.tick_y(5)
    dn.tick_b(3)
    dn.tick_y(0)
    phase("n1")
    norms.forward(1)
    phase("a6")
    gu.tick_a(6, 0)
    dn.tick_a(3, 0)
    gu.tick_a(6, 1)
    dn.tick_a(3, 1)
    norms.last(0)
    phase("b8")
    gu.tick_b(8)
    gu.tick_y(6)
    dn.tick_b(4, along_y=False)
    norms.last(1)
    phase("a7")
    gu.tick_a(7, 0)
    dn.tick_a(4, 0)
    gu.tick_y(7)
    gu.tick_a(7, 1)
    dn.tick_a(4, 1)
    gu.tick_y(8)
    dn.start_y(4)
    dn.tick_y(1)
    dn.tick_b(5)
    dn.tick_y(2)
    phase("n_fin")
    norms.finish(0)
    norms.finish(1)
    for s in range(0, 7):
        gu.finish(s)
    phase("early0")
    up_early(0)
    up_early(1)
    phase("a8")
    gu.tick_a(8, 0)
    dn.tick_a(5, 0)
    phase("early1")
    up_early(2)
    phase("early2")
    up_early(3)
    up_early(4)
    acc[:, 1280:1408] = up_dot(0, EARLY, 1280)
    phase("a8b")
    gu.tick_a(8, 1)
    dn.tick_a(5, 1)
    dn.tick_b(6)
    dn.tick_y(3)
    phase("g_fin")
    for s in range(7, HALF + 1):
        gu.finish(s)

    phase("up0")
    for j in range(4):
        up_step(j)
    phase("d6")
    dn.tick_a(6, 0)
    dn.tick_a(6, 1)
    dn.tick_b(7)
    dn.tick_y(4)
    phase("up2")
    up_step(4)
    v = acc[:, 1280:1408] + up_dot(EARLY, NZ, 1280)
    v = v / (1.0 + jnp.exp(-v)) * pltpu.roll(v, 64, 1)
    low = lax.broadcasted_iota(jnp.int32, (TOK, 128), 1) < 64
    hid[:, 640:768] = jnp.where(low, v, 0.0).astype(BF16)

    def weights_of(zb):
        v = wdn[pl.ds(zb * NY, NY)]
        main = jnp.concatenate([v[:, :, 0:640], v[:, :, 640:1280]], axis=1).reshape(128, 640)
        tail = v[:, :, 1280:1408]
        turned = pltpu.roll(tail.reshape(64, 128).astype(F32), 64, 1).astype(BF16)
        tail = jnp.concatenate([tail, turned.reshape(NY, 16, 128)], axis=1).reshape(128, 128)
        return jnp.concatenate([main, tail], axis=1)

    def place(o):
        s = o // 2 + 1
        if s == HALF:
            return (z + HALF * (o % 2)) % NZ
        return (z + (s if o % 2 else NZ - s)) % NZ

    def down_step(i):
        w = jnp.concatenate([weights_of(place(2 * i)), weights_of(place(2 * i + 1))], axis=0)
        v = dot_t(hid[...], w)
        part[:, :, i * 256 : (i + 1) * 256] = v.astype(BF16).reshape(NT, ROWS, 256)

    xs = (net.x2, net.xm, net.xp, net.x)

    def span(k):
        return pl.ds(SPANS[k][0] * 256, (SPANS[k][1] - SPANS[k][0]) * 256)

    def sum_start(k):
        for i, xb in enumerate(xs):
            send(part.at[xb * 2 + net.other, :, span(k)], pr.at[xb, :, span(k)],
                 p_send.at[4 * k + i], p_recv.at[NX * k + xb], tp=net.tpo)

    def pair(k, xb):
        arrived(pr.at[xb, :, span(k)], p_send.at[0], p_recv.at[NX * k + xb], tp=net.tpo)
        mine = part[xb * 2 + net.c, :, span(k)].astype(F32)
        return mine + pr[xb, :, span(k)].astype(F32)

    def hop(k, i, value, to):
        ps[i, :, span(k)] = value.astype(BF16)
        send(ps.at[i, :, span(k)], rs.at[i, :, span(k)],
             r_send.at[3 * k + i], r_recv.at[3 * k + i], tp=to)

    def landed(k, i, frm):
        arrived(rs.at[i, :, span(k)], r_send.at[0], r_recv.at[3 * k + i], tp=frm)
        return rs[i, :, span(k)].astype(F32)

    def sum_pair(k):
        hop(k, 0, pair(k, net.x2), net.tp2 if k >= STRAIGHT else net.tpp)
        hop(k, 1, pair(k, net.xm), net.tpm)
        if k >= STRAIGHT:
            hop(k, 2, pair(k, net.xp), net.tpp)

    def sum_relay(k):
        if k >= STRAIGHT:
            return
        near = pair(k, net.xp)
        hop(k, 2, near + landed(k, 0, net.tpm), net.tpp)

    def sum_finish(k):
        total = pair(k, net.x) + landed(k, 1, net.tpp) + landed(k, 2, net.tpm)
        if k >= STRAIGHT:
            total = total + landed(k, 0, net.tp2)
        total = total.astype(BF16)
        for i in range(2 * (SPANS[k][1] - SPANS[k][0])):
            cols = pl.ds(pl.multiple_of(place(2 * SPANS[k][0] + i) * 128, 128), 128)
            out_ref[:, cols] = total[:, i * 128 : (i + 1) * 128]

    phase("w0")
    dn.finish(1)
    down_step(0)
    dn.finish(2)
    down_step(1)
    sum_start(0)
    phase("d7")
    dn.tick_a(7, 0)
    dn.tick_a(7, 1)
    dn.tick_b(8)
    dn.tick_y(5)
    dn.tick_y(6)
    phase("w2")
    dn.finish(3)
    down_step(2)
    sum_pair(0)
    dn.finish(4)
    down_step(3)
    sum_start(1)
    phase("d8")
    dn.tick_a(8, 0)
    dn.tick_a(8, 1)
    dn.tick_y(7)
    dn.tick_y(8)
    phase("w4")
    dn.finish(5)
    down_step(4)
    sum_pair(1)
    phase("w5")
    dn.finish(6)
    down_step(5)
    sum_start(2)
    sum_relay(0)
    phase("w6")
    dn.finish(7)
    down_step(6)
    sum_pair(2)
    phase("w7")
    dn.finish(0)
    dn.finish(8)
    down_step(7)
    sum_start(3)
    phase("relay1")
    sum_relay(1)
    sum_pair(3)
    phase("rs0")
    sum_relay(2)
    sum_finish(0)
    phase("rs1")
    sum_finish(1)
    phase("rs2")
    sum_finish(2)
    phase("rs3")
    sum_finish(3)

    phase("drain")
    keep.wait()
    for cp in net.sent:
        cp.wait_send()
    for k in range(1, NZ):

        @pl.when(z + k < NZ)
        def _():
            net.copy(tb.at[z], tb.at[z], t_send.at[k], t_recv.at[z], sp_0=(z + k) % NZ).wait_send()

    phase(None)


def on_device(
    mixer_in, residual, decay_real, decay_imag, log_step, in_real, in_imag,
    output_real, output_imaginary, skip, out_proj, norm_gain, w_gate, w_up, w_down,
):
    vmem = pltpu.VMEM
    dma = pltpu.SemaphoreType.DMA
    scratch = [
        vmem((TOK, CHD), BF16),
        vmem((8, 64), F32),
        vmem((8, 64), F32),
        vmem((1, 8), F32),
        vmem((CHD, 64), F32),
        vmem((CHD, 64), F32),
        vmem((CHD, 64), F32),
        vmem((CHD, 64), F32),
        vmem((1, CHD), F32),
        vmem((1, D), F32),
        vmem((ROWS, D), BF16),
        vmem((32, FFD), BF16),
        vmem((32, FFD), BF16),
        vmem((32, FFD), BF16),
        vmem((NZ * NY, 32, GU), BF16),
        vmem((NZ * NY, 16, GU), BF16),
        vmem((NT, CHD, D), BF16),
        vmem((NY, 8, 128), F32),
        vmem((NZ, 8, 128), F32),
        vmem((NT, ROWS, CHD), BF16),
        vmem((NT, ROWS, CHD), BF16),
        vmem((NT, ROWS, D), BF16),
        vmem((TOK, 768), BF16),
        vmem((NT, ROWS, D), BF16),
        vmem((NX, ROWS, D), BF16),
        vmem((3, ROWS, D), BF16),
        vmem((3, ROWS, D), BF16),
        vmem((TOK, FL), F32),
        vmem((TOK, FL), F32),
        vmem((2, CHD, FL), BF16),
        vmem((2, CHD, FL), BF16),
        vmem((64, FL), F32),
        vmem((64, FL), F32),
        vmem((64, FL), F32),
        vmem((64, FL), F32),
        vmem((ROWS, D), F32),
        vmem((TOK, GU), F32),
    ]
    counts = RING_SEMS + RING_SEMS + [
        2 * NT, 14, 2 * NT, 14, NY, NY, NZ, NZ, NT, NT, NC * NX, NC * 4, NC * 3, NC * 3, 16,
    ]
    scratch += [dma((n,)) for n in counts]
    carried, down = pl.pallas_call(
        kernel,
        out_shape=(jax.ShapeDtypeStruct((ROWS, D), F32), jax.ShapeDtypeStruct((ROWS, D), BF16)),
        in_specs=[pl.BlockSpec(memory_space=pl.ANY)] * 15,
        out_specs=(pl.BlockSpec(memory_space=pl.ANY), pl.BlockSpec(memory_space=vmem)),
        scratch_shapes=scratch,
        compiler_params=pltpu.CompilerParams(
            collective_id=0, has_side_effects=True, vmem_limit_bytes=60 * 1024 * 1024
        ),
    )(
        mixer_in, decay_real, decay_imag, log_step.reshape(1, 8),
        jnp.transpose(in_real, (0, 2, 1)).reshape(CHD, 64),
        jnp.transpose(in_imag, (0, 2, 1)).reshape(CHD, 64),
        output_real.reshape(CHD, 64), output_imaginary.reshape(CHD, 64),
        skip.reshape(1, CHD), out_proj, norm_gain.reshape(1, D),
        residual, w_gate, w_up, w_down.T,
    )
    return (carried + 0.5 * down.astype(F32)).astype(BF16)


def solution(mesh):
    finer = Mesh(mesh.devices.reshape(NZ, NY, mesh.shape["tp"]), ("sp_0", "sp_1", "tp"))
    return jax.shard_map(
        on_device,
        mesh=finer,
        in_specs=(
            P(SP, "tp"),
            P(SP_TP, None),
            P("tp", None),
            P("tp", None),
            P("tp"),
            P("tp", None, None),
            P("tp", None, None),
            P("tp", None, None),
            P("tp", None, None),
            P("tp"),
            P("tp", None),
            P(),
            P(SP, "tp"),
            P(SP, "tp"),
            P("tp", SP),
        ),
        out_specs=P(SP_TP, None),
        check_vma=False,
    )
```
